128 devices in a mesh: sp: 16 (over z, x), dp: 8 (over y, core).
Axes of the slice: x: 4, y: 4, z: 4, core: 2. Of those that a mesh axis runs over, the one named last changes fastest.
Arguments:
- resid: bfloat16 [8, 4096, 2048], P('dp', 'sp'), may hold values from -4 to 4
- query: bfloat16 [8, 4096, 2048], P('dp', 'sp'), may hold values from -6 to 6
- keys: bfloat16 [8, 4096, 512], P('dp', 'sp'), may hold values from -6 to 6
- values: bfloat16 [8, 4096, 512], P('dp', 'sp'), may hold values from -6 to 6
- q_gain: float32 [128], replicated, may hold values from 0.7 to 5
- k_gain: float32 [128], replicated, may hold values from 0.7 to 5
- out_weight: bfloat16 [2048, 2048], P('dp'), may hold values from -0.5 to 0.5
- norm_gain: float32 [2048], replicated, may hold values from 0.1 to 1.9
- route_ids: int32 [8, 4096, 2], P('dp', 'sp'), may hold values from 0 to 127, all different within a row; in each aligned block of 256 rows (0 to 255, 256 to 511, ..., all dimensions but the last counted through in order) at most 6 rows name the same one
- route_weight: float32 [8, 4096, 2], P('dp', 'sp'), may hold values from 0.2 to 1
- expert_gate: bfloat16 [128, 2048, 1024], P(('sp', 'dp')), may hold values from -0.125 to 0.125
- expert_up: bfloat16 [128, 2048, 1024], P(('sp', 'dp')), may hold values from -0.125 to 0.125
- expert_down: bfloat16 [128, 1024, 2048], P(('sp', 'dp')), may hold values from -0.1875 to 0.1875
Outputs:
- layer_out: bfloat16 [8, 4096, 2048], P('dp', 'sp')
The draws below stay inside these ranges and needn't reach their ends.
Inputs may be any that keep to these rules, and one draw needn't show every extreme that they name: `route_ids`: each row names 2 different experts. In the rows of one device no expert is named more than 6 times, and in some devices some expert is named exactly 6 times.
All inputs are finite; a program needn't handle non-finite values.
Results may differ from the reference program's by a relative error of at most 0.0095.
The reference program's roundings to bfloat16 on the way count: a program that leaves them out, or rounds other values in their place, can miss the bound.
Values may be sent and summed in bfloat16 or wider, within the bound.
A program may use at most 128 MiB of HBM per device.

```python
import math
import jax
import jax.numpy as jnp
import numpy as np
from jax import lax

D = 2048
QH = 16
KVH = 4
HD = 128
FE = 1024
TOP = 2
GRID_W = 64
TOK_DEV = 256
LEN = 4096
SEQS = 8
EXPERTS = 128
CAP = 6
N_SP = 16
N_DP = 8


def drawn_keys(key):
    return jnp.clip(jax.random.normal(jax.random.fold_in(key, 31), (SEQS, LEN, KVH * HD), jnp.float32), -6.0, 6.0)


def draw_keys(key, part):
    return drawn_keys(key).astype(jnp.bfloat16)


def draw_query(key, part):
    base = jnp.clip(jax.random.normal(jax.random.fold_in(key, 32), (SEQS, LEN, QH * HD), jnp.float32), -6.0, 6.0)
    return base.astype(jnp.bfloat16)


def gain_draw(key, salt):
    return jax.random.uniform(jax.random.fold_in(key, salt), (HD,), jnp.float32, 0.7, 1.6)


def draw_q_gain(key, part):
    return gain_draw(key, 41)


def draw_k_gain(key, part):
    return gain_draw(key, 42)


def block_levels(key, shape, split, low, high):
    factor_of, own = 1.0, jax.random.fold_in(key, 6)
    for position, parts in split:
        heights = jnp.exp(jax.random.uniform(jax.random.fold_in(own, position), (parts,), jnp.float32, low / len(split), high / len(split)))
        factor_of = factor_of * jnp.repeat(heights, shape[position] // parts).reshape([-1 if axis == position else 1 for axis in range(len(shape))])
    return factor_of


def routed_block(rng, own, number, rows, count, top, limit, slope):
    order = jax.random.permutation(rng, count)
    packed, ordinary = shares(count, rows * top, limit, slope, True), shares(count, rows * top, limit, slope, False)
    places = jnp.arange(count)

    def named(sizes, turn):
        used = int((sizes > 0).sum())
        fixed = max(1, used // 4)
        moved = fixed + (places - fixed + turn * (used - fixed)) % max(1, count - fixed)
        return jnp.zeros((count,), jnp.int32).at[order[jnp.where(places < fixed, places, moved)]].set(jnp.asarray(sizes, jnp.int32))

    sizes = jnp.where(number % 4 == 0, named(packed, number // 4), named(ordinary, number - number // 4 - 1))
    mixed = jax.random.permutation(jax.random.fold_in(own, 3), count)
    giver, sink = mixed[0:count // 2 * 2:2], mixed[1:count // 2 * 2:2]
    room = jnp.minimum(sizes[giver] - 1, limit - sizes[sink]) // 2
    room = jnp.where((giver == order[0]) | (sink == order[0]) | (sizes[sink] == 0), 0, jnp.maximum(room, 0))
    moved = jax.random.randint(jax.random.fold_in(own, 4), (count // 2,), 0, 1 << 20) % (room + 1)
    sizes = sizes.at[giver].add(-moved).at[sink].add(moved)
    labels = jnp.searchsorted(jnp.cumsum(sizes), jnp.arange(rows * top), side="right").astype(jnp.int32)
    grid = labels.reshape(top, rows).T
    grid = grid[jax.random.permutation(jax.random.fold_in(own, 1), rows)]
    turn = jax.random.randint(jax.random.fold_in(own, 2), (rows, 1), 0, top)
    return jnp.take_along_axis(grid, (jnp.arange(top)[None, :] + turn) % top, axis=1)


def shares(amount, total, bound, lean, full):
    weights = [(1 << 20) // math.isqrt(rank ** lean) + 1 for rank in range(1, amount + 1)]
    largest = bound if full else min(bound, max(-(-total // amount), total * weights[0] // sum(weights)))
    least = 1 if total - largest >= amount - 1 else 0
    given, spare = [largest] + [least] * (amount - 1), total - largest - least * (amount - 1)
    while spare > 0:
        candidates = [i for i in range(1, amount) if given[i] < largest] or [i for i in range(1, amount) if given[i] < bound]
        whole, left = sum([weights[i] for i in candidates]), spare
        for i in candidates:
            extra = min(bound - given[i], max(1, left * weights[i] // whole), spare)
            given[i] = given[i] + extra
            spare = spare - extra
    return np.array(given)


def scatter_about(rng, dims, width, most, split=(), kind=jnp.bfloat16):
    array = jax.random.normal(rng, dims, jnp.float32) * width
    if len(split) > 0:
        array = block_levels(rng, dims, split, -0.22, 0.18) * array
    return jnp.clip(array, min=-most, max=most).astype(kind)


def setup_inputs(seed: int = 0) -> dict:
    seeds = jax.random.split(jax.random.key(seed), 14)
    resid = scatter_about(seeds[0], (SEQS, LEN, D), 0.5, 4.0, ((0, 8), (1, 16)))
    query = draw_query(jax.random.fold_in(seeds[13], 71), 0)
    keys = draw_keys(jax.random.fold_in(seeds[13], 71), 0)
    values = scatter_about(seeds[3], (SEQS, LEN, KVH * HD), 1.0, 6.0, ((0, 8), (1, 16)))
    q_gain = draw_q_gain(jax.random.fold_in(seeds[13], 71), 0)
    k_gain = draw_k_gain(jax.random.fold_in(seeds[13], 71), 0)
    out_weight = scatter_about(seeds[6], (QH * HD, D), HD ** -0.5, 0.5, ((0, 8),))
    norm_gain = jnp.clip(1.0 + 0.18 * jax.random.normal(seeds[7], (D,), jnp.float32), 0.1, 1.9)
    route_ids_keys = jax.random.split(jax.random.fold_in(seeds[8], 1), SEQS * LEN // TOK_DEV)
    route_ids_turns = jax.random.permutation(jax.random.fold_in(seeds[8], 3), SEQS * LEN // TOK_DEV)
    route_ids = jax.vmap(lambda own, number: routed_block(jax.random.fold_in(seeds[8], 2), own, number, TOK_DEV, EXPERTS, TOP, CAP, 2))(route_ids_keys, route_ids_turns).reshape((SEQS, LEN, TOP))
    route_weight = jnp.clip(0.2 + 0.8 * jax.random.uniform(seeds[9], (SEQS, LEN, TOP), jnp.float32) ** block_levels(seeds[9], (SEQS, LEN, TOP), ((0, 8), (1, 16)), -0.2, 0.2), 0.2, 1.0)
    expert_gate = scatter_about(seeds[10], (EXPERTS, D, FE), D ** -0.5, 0.125, ((0, 128),))
    expert_up = scatter_about(seeds[11], (EXPERTS, D, FE), D ** -0.5, 0.125, ((0, 128),))
    expert_down = scatter_about(seeds[12], (EXPERTS, FE, D), FE ** -0.5, 0.1875, ((0, 128),))
    return {"resid": resid, "query": query, "keys": keys, "values": values, "q_gain": q_gain, "k_gain": k_gain, "out_weight": out_weight, "norm_gain": norm_gain, "route_ids": route_ids, "route_weight": route_weight, "expert_gate": expert_gate, "expert_up": expert_up, "expert_down": expert_down}


EPSILON = 1e-06
THETA = 10000.0
LIMIT = 7.0
SLOPE = 1.702

def turn_half(matrix, places):
    half_width = matrix.shape[-1] // 2
    inverse = THETA ** (-jnp.arange(half_width, dtype=jnp.float32) / half_width)
    angles = places.astype(jnp.float32)[:, None] * inverse[None, :]
    cosine = jnp.cos(angles)[:, None, :]
    sine_part = jnp.sin(angles)[:, None, :]
    leading = matrix[..., :half_width]
    second = matrix[..., half_width:]
    return jnp.concatenate([leading * cosine - second * sine_part, second * cosine + leading * sine_part], axis=-1)

def prepare(projected_rows, gain_vector, head_count, places):
    matrix = projected_rows.astype(jnp.float32).reshape(projected_rows.shape[0], head_count, -1)
    matrix = matrix * lax.rsqrt(lax.optimization_barrier(jnp.mean(matrix * matrix, axis=-1, keepdims=True)) + EPSILON) * gain_vector
    middle = matrix.shape[-1] // 2
    turned = jnp.concatenate([turn_half(matrix[..., :middle], places // GRID_W), turn_half(matrix[..., middle:], places % GRID_W)], axis=-1)
    return turned.astype(jnp.bfloat16)

def attend(head_query, head_key, head_value):
    length, local_heads, head_dim = head_query.shape
    local_kv = head_key.shape[1]
    group_size = local_heads // local_kv
    block_rows = min(512, length)
    scaling = head_dim ** (-0.5)
    query_blocks = head_query.reshape(length // block_rows, block_rows, local_kv, group_size, head_dim)
    key_wide = head_key.astype(jnp.float32)
    value_wide = head_value.astype(jnp.float32)

    def one_block(query_block):
        scores = jnp.einsum('qkgd,skd->kgqs', query_block.astype(jnp.float32), key_wide) * scaling
        lifted = jnp.exp(scores - lax.optimization_barrier(jnp.max(scores, axis=-1, keepdims=True)))
        attn_weights = (lifted / lax.optimization_barrier(jnp.sum(lifted, axis=-1, keepdims=True))).astype(jnp.bfloat16)
        return jnp.einsum('kgqs,skd->qkgd', attn_weights.astype(jnp.float32), value_wide).astype(jnp.bfloat16)
    return lax.map(one_block, query_blocks).reshape(length, local_heads, head_dim)

def apply_expert(batch, gate_matrix, up_matrix, down_matrix):
    flat_rows = batch.reshape(-1, batch.shape[-1])
    gated = jnp.minimum(jnp.dot(flat_rows, gate_matrix, preferred_element_type=jnp.float32), LIMIT)
    linear = jnp.clip(jnp.dot(flat_rows, up_matrix, preferred_element_type=jnp.float32), -LIMIT, LIMIT)
    active = (gated * jax.nn.sigmoid(SLOPE * gated) * (linear + 1.0)).astype(jnp.bfloat16)
    return jnp.dot(active, down_matrix, preferred_element_type=jnp.float32).astype(jnp.bfloat16).reshape(batch.shape)

def block_tables(block_ids, block_weights):
    chosen = block_ids.reshape(-1)
    onehot = (chosen[:, None] == jnp.arange(EXPERTS, dtype=jnp.int32)[None, :]).astype(jnp.int32)
    earlier = lax.optimization_barrier(jnp.sum((jnp.cumsum(onehot, axis=0) - onehot) * onehot, axis=1))
    target = (chosen * CAP + earlier).astype(jnp.int32)
    sources = jnp.arange(TOK_DEV * TOP, dtype=jnp.int32) // TOP
    slot_table = jnp.full((EXPERTS * CAP,), -1, jnp.int32).at[target].set(sources)
    slot_weight = jnp.zeros((EXPERTS * CAP,), jnp.float32).at[target].set(block_weights.reshape(-1))
    return (slot_table, slot_weight)

def reference(resid, query, keys, values, q_gain, k_gain, out_weight, norm_gain, route_ids, route_weight, expert_gate, expert_up, expert_down):
    places = jnp.arange(LEN, dtype=jnp.int32)

    def one_sequence(operands):
        query_rows, key_rows, value_rows = operands
        query_turned = prepare(query_rows, q_gain, QH, places)
        key_turned = prepare(key_rows, k_gain, KVH, places)
        mixed = attend(query_turned, key_turned, value_rows.reshape(LEN, KVH, HD))
        return mixed.reshape(LEN, QH * HD)
    head_out = lax.map(one_sequence, (query, keys, values))
    projected = jnp.dot(head_out.reshape(SEQS * LEN, QH * HD), out_weight, preferred_element_type=jnp.float32)
    updated = (resid.reshape(SEQS * LEN, D).astype(jnp.float32) + projected).astype(jnp.bfloat16)
    widened = updated.astype(jnp.float32)
    normed = (widened * lax.rsqrt(lax.optimization_barrier(jnp.mean(widened * widened, axis=-1, keepdims=True)) + EPSILON) * norm_gain).astype(jnp.bfloat16)
    block_count = N_SP * N_DP
    slot_table, slot_weight = jax.vmap(block_tables)(route_ids.reshape(block_count, TOK_DEV, TOP), route_weight.reshape(block_count, TOK_DEV, TOP))
    slot_table = jnp.transpose(slot_table.reshape(block_count, EXPERTS, CAP), (1, 0, 2))
    slot_weight = jnp.transpose(slot_weight.reshape(block_count, EXPERTS, CAP), (1, 0, 2))
    block_start = (jnp.arange(block_count, dtype=jnp.int32) * TOK_DEV)[:, None]

    def one_expert(running, operands):
        gate_matrix, up_matrix, down_matrix, table_rows, weight_rows = operands
        valid = table_rows >= 0
        global_rows = jnp.where(valid, table_rows + block_start, 0).reshape(-1).astype(jnp.int32)
        answered = apply_expert(normed[global_rows], gate_matrix, up_matrix, down_matrix)
        scaled = answered.astype(jnp.float32) * jnp.where(valid, weight_rows, 0.0).reshape(-1)[:, None]
        return (running.at[global_rows].add(scaled), None)
    combined = lax.scan(one_expert, jnp.zeros((SEQS * LEN, D), jnp.float32), (expert_gate, expert_up, expert_down, slot_table, slot_weight))[0]
    return (widened + combined).astype(jnp.bfloat16).reshape(SEQS, LEN, D)
```

```python
import functools
import jax
import jax.numpy as jnp
from jax import lax
from jax.experimental import pallas as pl
from jax.experimental.pallas import tpu as pltpu
from jax.sharding import PartitionSpec as P

GRID_W = 64
EPSILON = 1e-06
THETA = 10000.0
LIMIT = 7.0
SLOPE = 1.702
LOG2E = 1.4426950408889634
HD = 128
TOK = 256
ZN = 4
XN = 4
N_DEV = 128
CAP = 6
BF = jnp.bfloat16
F32 = jnp.float32
MESH = pl.DeviceIdType.MESH
VM = pl.BlockSpec(memory_space=pltpu.VMEM)
SM = pl.BlockSpec(memory_space=pltpu.SMEM)
MB = 1 << 20


def params(limit=48 * MB, cid=None, **kw):
    if cid is not None:
        kw.update(collective_id=cid, has_side_effects=True)
    return pltpu.CompilerParams(vmem_limit_bytes=limit, **kw)


def turn_tables(places):
    lane = jnp.arange(HD, dtype=jnp.int32)
    inverse = THETA ** (-(lane % 32).astype(F32) / 32)
    place = jnp.where(lane[None, :] < 64, (places // GRID_W)[:, None], (places % GRID_W)[:, None])
    angles = place.astype(F32) * inverse[None, :]
    sign = jnp.where(lane % 64 < 32, -1.0, 1.0)
    return jnp.cos(angles), jnp.sin(angles) * sign[None, :]


def turn_head(x, gain, cosine, sine, first):
    x = x.astype(F32)
    x = x * lax.rsqrt(jnp.mean(x * x, axis=-1, keepdims=True) + EPSILON) * gain
    other = jnp.where(first, pltpu.roll(x, HD - 32, 1), pltpu.roll(x, 32, 1))
    return (x * cosine + other * sine).astype(BF)


def prep_kernel(q_ref, k_ref, v_ref, qg_ref, kg_ref, cos_ref, sin_ref, idr_ref, idc_ref,
                qs_ref, kvs_ref, tgt_ref, slot_ref):
    first = lax.broadcasted_iota(jnp.int32, (TOK, HD), 1) % 64 < 32
    cosine, sine = cos_ref[...], sin_ref[...]
    for h in range(16):
        qs_ref[h // 4, :, (h % 4) * HD:(h % 4 + 1) * HD] = turn_head(
            q_ref[:, h * HD:(h + 1) * HD], qg_ref[...], cosine, sine, first)
    for h in range(4):
        kvs_ref[h, 0] = turn_head(k_ref[:, h * HD:(h + 1) * HD], kg_ref[...], cosine, sine, first)
        kvs_ref[h, 1] = v_ref[:, h * HD:(h + 1) * HD]
    n = 2 * TOK
    row, col = idr_ref[...], idc_ref[...]
    ia = lax.broadcasted_iota(jnp.int32, (n, n), 0)
    ib = lax.broadcasted_iota(jnp.int32, (n, n), 1)
    same = col == row
    before = jnp.sum(jnp.where(same & (ia < ib), 1.0, 0.0), axis=0, keepdims=True)
    tgt_ref[...] = row * CAP + before.astype(jnp.int32)
    before_c = jnp.sum(jnp.where(same & (ib < ia), 1.0, 0.0), axis=1, keepdims=True)
    target = col * CAP + before_c.astype(jnp.int32)
    slots = lax.broadcasted_iota(jnp.int32, (n, N_DEV * CAP), 1)
    token = (lax.broadcasted_iota(jnp.int32, (n, N_DEV * CAP), 0) // 2).astype(F32)
    slot_ref[...] = jnp.sum(jnp.where(target == slots, token, 0.0), axis=0, keepdims=True).astype(jnp.int32)


def sp_of(z, x):
    return {"sp": lax.rem(z, ZN) * XN + lax.rem(x, XN)}


def spread_kernel(qs_ref, kvs_ref, q_ref, kv_ref, zks, zkr, zqs, zqr, xs, xr, fs, fr):
    sp = lax.axis_index("sp")
    z, x = sp // XN, lax.rem(sp, XN)
    bar = pltpu.get_barrier_semaphore()
    for d in (1, 2, 3):
        pl.semaphore_signal(bar, inc=1, device_id=sp_of(z + d, x), device_id_type=MESH)
    for d in (1, 3):
        pl.semaphore_signal(bar, inc=1, device_id=sp_of(z, x + d), device_id_type=MESH)
    pl.semaphore_wait(bar, 5)
    pending = []

    def send(src, dst, ssem, rsem, dev):
        c = pltpu.make_async_remote_copy(src, dst, ssem, rsem, device_id=dev, device_id_type=MESH)
        c.start()
        pending.append(c)
        return c

    zk = {}
    for d in (1, 3, 2):
        zk[d] = send(kvs_ref.at[lax.rem(z + d, ZN)], kv_ref.at[x, z], zks.at[d - 1], zkr.at[d - 1], sp_of(z + d, x))
    kv_ref[x, z] = kvs_ref[z]

    def gather(d):
        chunk = lax.rem(z + ZN - d, ZN)
        return [send(kv_ref.at[x, chunk], kv_ref.at[x, chunk], xs.at[s, d], xr.at[s, d], sp_of(z, x + (1, 3)[s])) for s in (0, 1)]

    near = {0: gather(0)}
    zq = {}
    for d in (1, 3, 2):
        zq[d] = send(qs_ref.at[lax.rem(z + d, ZN)], q_ref.at[z], zqs.at[d - 1], zqr.at[d - 1], sp_of(z + d, x))
    q_ref[z] = qs_ref[z]
    far = []

    def forward(d):
        chunk = lax.rem(z + ZN - d, ZN)
        s = 0 if d in (0, 1) else 1
        near[d][s].wait_recv()
        came = lax.rem(x + (3, 1)[s], XN)
        far.append(send(kv_ref.at[came, chunk], kv_ref.at[came, chunk], fs.at[d], fr.at[d], sp_of(z, x + (1, 3)[s])))

    prev = 0
    for d in (1, 3, 2):
        zk[d].wait_recv()
        near[d] = gather(d)
        forward(prev)
        prev = d
    forward(prev)
    for d in (0, 1, 2, 3):
        s = 0 if d in (0, 1) else 1
        near[d][1 - s].wait_recv()
    for d in (1, 3, 2):
        zq[d].wait_recv()
    for c in far:
        c.wait_recv()
    for c in pending:
        c.wait_send()


def attend_kernel(q_ref, kv_ref, o_ref, ve_ref):
    scale = HD ** -0.5 * LOG2E

    @pl.when(pl.program_id(0) == 0)
    def _():
        lane = lax.broadcasted_iota(jnp.int32, (1024, HD), 1)
        for c in range(4):
            ve_ref[c * 1024:(c + 1) * 1024, :HD] = kv_ref[c, :, 1].reshape(1024, HD)
            ve_ref[c * 1024:(c + 1) * 1024, HD:] = jnp.where(lane == 0, 1.0, 0.0).astype(BF)

    q = q_ref[0]
    m = acc = None
    for c in range(4):
        k = kv_ref[c, :, 0].reshape(1024, HD)
        s = lax.dot_general(q, k, (((1,), (1,)), ((), ())), preferred_element_type=F32)
        top = jnp.max(s, axis=-1, keepdims=True) * scale
        m_new = top if m is None else jnp.maximum(m, top)
        p = jnp.exp2(s * scale - m_new).astype(BF)
        part = jnp.dot(p, ve_ref[c * 1024:(c + 1) * 1024, :], preferred_element_type=F32)
        acc = part if acc is None else acc * jnp.exp2(m - m_new) + part
        m = m_new
    o_ref[0] = (acc[:, :HD] / acc[:, HD:HD + 1]).astype(BF)


def gather_kernel(o_ref, r_ref, ss, rs):
    sp = lax.axis_index("sp")
    z, x = sp // XN, lax.rem(sp, XN)
    bar = pltpu.get_barrier_semaphore()
    for d in (1, 2, 3):
        pl.semaphore_signal(bar, inc=1, device_id=sp_of(z + d, x), device_id_type=MESH)
    pl.semaphore_wait(bar, 3)
    cs = []
    for d in (1, 3, 2):
        c = pltpu.make_async_remote_copy(o_ref.at[lax.rem(z + d, ZN)], r_ref.at[z], ss.at[d - 1], rs.at[d - 1],
                                         device_id=sp_of(z + d, x), device_id_type=MESH)
        c.start()
        cs.append(c)
    r_ref[z] = o_ref[z]
    for c in cs:
        c.wait()


def project_kernel(slot_ref, t_ref, w_ref, r_ref, g_ref, u_ref, out_ref, u2, sq, n3):
    i = pl.program_id(0)
    nb = w_ref.shape[1]
    y = r_ref[...].astype(F32)
    acc = jnp.dot(t_ref[0], w_ref[0:512, :], preferred_element_type=F32)
    for k in range(1, 4):
        acc = acc + jnp.dot(t_ref[k], w_ref[k * 512:(k + 1) * 512, :], preferred_element_type=F32)
    u = (y + acc).astype(BF)
    u_ref[...] = u
    wide = u.astype(F32)
    u2[i] = wide
    part = jnp.sum(wide * wide, axis=-1, keepdims=True)

    @pl.when(i == 0)
    def _():
        sq[...] = part

    @pl.when(i > 0)
    def _():
        sq[...] += part

    @pl.when(i == pl.num_programs(0) - 1)
    def _():
        inv = lax.rsqrt(sq[...] / 2048.0 + EPSILON)
        per = nb // HD
        for j in range(16):
            piece = u2[j // per, :, (j % per) * HD:(j % per + 1) * HD]
            n3[:, j, :] = (piece * inv * g_ref[:, j * HD:(j + 1) * HD]).astype(BF).astype(F32)

        def slot(s, _):
            out_ref[s] = n3[slot_ref[0, s]].astype(BF)
            return 0

        lax.fori_loop(0, N_DEV * CAP, slot, 0, unroll=8)


def swap_kernel(a_ref, b_ref, ss, rs):
    me = lax.axis_index("sp") * 8 + lax.axis_index("dp")
    bar = pltpu.get_barrier_semaphore()

    def dev(p):
        return {"sp": p // 8, "dp": lax.rem(p, 8)}

    def sig(i, _):
        pl.semaphore_signal(bar, inc=1, device_id=dev(lax.rem(me + i, N_DEV)), device_id_type=MESH)
        return 0

    lax.fori_loop(1, N_DEV, sig, 0)
    pl.semaphore_wait(bar, N_DEV - 1)

    def send(i, _):
        p = lax.rem(me + i * 37, N_DEV)
        pltpu.make_async_remote_copy(a_ref.at[p], b_ref.at[me], ss, rs, device_id=dev(p), device_id_type=MESH).start()
        return 0

    lax.fori_loop(1, N_DEV, send, 0)
    b_ref[me] = a_ref[me]
    rest = pl.ds(0, N_DEV - 1)
    pltpu.make_async_remote_copy(a_ref.at[rest], b_ref.at[rest], ss, rs, device_id=dev(me), device_id_type=MESH).wait()


def expert_kernel(x_ref, wg_ref, wu_ref, wd_ref, y_ref, w3, xs, act):
    i = pl.program_id(0)
    n = N_DEV * CAP

    @pl.when(i == 0)
    def _():
        def widen(t, _):
            rows = pl.ds(t * 8, 8)
            w3[rows] = x_ref[rows].astype(F32)
            return 0

        lax.fori_loop(0, n // 8, widen, 0, unroll=2)
        for j in range(16):
            xs[:, j * HD:(j + 1) * HD] = w3[:, j, :].astype(BF)

    @pl.when(i < 4)
    def _():
        x = xs[...]
        g = jnp.minimum(jnp.dot(x, wg_ref[...], preferred_element_type=F32), LIMIT)
        l = jnp.clip(jnp.dot(x, wu_ref[...], preferred_element_type=F32), -LIMIT, LIMIT)
        act[i] = (g * jax.nn.sigmoid(SLOPE * g) * (l + 1.0)).astype(BF)

    @pl.when(i >= 4)
    def _():
        y = jnp.dot(act[0], wd_ref[0:256, :], preferred_element_type=F32)
        for k in range(1, 4):
            y = y + jnp.dot(act[k], wd_ref[k * 256:(k + 1) * 256, :], preferred_element_type=F32)
        y = y.astype(BF).astype(F32)
        for jj in range(4):
            w3[:, (i - 4) * 4 + jj, :] = y[:, jj * HD:(jj + 1) * HD]

    @pl.when(i == 7)
    def _():
        def narrow(t, _):
            rows = pl.ds(t * 8, 8)
            y_ref[rows] = w3[rows].astype(BF)
            return 0

        lax.fori_loop(0, n // 8, narrow, 0, unroll=2)


def combine_kernel(tgt_ref, wt_ref, y_ref, u_ref, o_ref, c3):
    def token(t, _):
        a = y_ref[tgt_ref[0, 2 * t]].astype(F32) * wt_ref[0, 2 * t]
        b = y_ref[tgt_ref[0, 2 * t + 1]].astype(F32) * wt_ref[0, 2 * t + 1]
        c3[t] = a + b
        return 0

    lax.fori_loop(0, TOK, token, 0, unroll=8)
    for j in range(16):
        cols = slice(j * HD, (j + 1) * HD)
        o_ref[:, cols] = (u_ref[:, cols].astype(F32) + c3[:, j, :]).astype(BF)


def full(shape):
    return pl.BlockSpec(shape, lambda *i: (0,) * len(shape))


def per_device(resid, query, keys, values, q_gain, k_gain, out_weight, norm_gain, route_ids, route_weight,
               expert_gate, expert_up, expert_down):
    sds = jax.ShapeDtypeStruct
    sem = pltpu.SemaphoreType.DMA
    weight = lax.all_gather(out_weight, "dp", axis=0, tiled=True)
    places = lax.axis_index("sp") * TOK + jnp.arange(TOK, dtype=jnp.int32)
    cosine, sine = turn_tables(places)
    ids = route_ids[0].reshape(1, 2 * TOK)
    qs, kvs, target, slots = pl.pallas_call(
        prep_kernel,
        out_shape=(sds((4, TOK, 512), BF), sds((4, 2, TOK, HD), BF), sds((1, 2 * TOK), jnp.int32),
                   sds((1, N_DEV * CAP), jnp.int32)),
        compiler_params=params(), name="prep",
    )(query[0], keys[0], values[0], q_gain[None], k_gain[None], cosine, sine, ids, ids.reshape(2 * TOK, 1))
    qr, kvr = pl.pallas_call(
        spread_kernel,
        out_shape=(sds((4, TOK, 512), BF), sds((4, 4, 2, TOK, HD), BF)),
        in_specs=[VM, VM], out_specs=(VM, VM),
        scratch_shapes=[sem((3,)), sem((3,)), sem((3,)), sem((3,)), sem((2, 4)), sem((2, 4)), sem((4,)), sem((4,))],
        compiler_params=params(cid=0), name="spread",
    )(qs, kvs)
    heads = pl.pallas_call(
        attend_kernel,
        grid=(16,),
        out_shape=sds((4, TOK, 512), BF),
        in_specs=[pl.BlockSpec((1, TOK, HD), lambda i: (i // 4, 0, i % 4)), full((4, 4, 2, TOK, HD))],
        out_specs=pl.BlockSpec((1, TOK, HD), lambda i: (i // 4, 0, i % 4)),
        scratch_shapes=[pltpu.VMEM((4096, 256), BF)],
        compiler_params=params(), name="attend",
        cost_estimate=pl.CostEstimate(flops=17_000_000_000, bytes_accessed=4_000_000, transcendentals=16_000_000),
    )(qr, kvr)
    tok = pl.pallas_call(
        gather_kernel,
        out_shape=sds((4, TOK, 512), BF),
        in_specs=[VM], out_specs=VM,
        scratch_shapes=[sem((3,)), sem((3,))],
        compiler_params=params(cid=1), name="heads_back",
    )(heads)
    nb = 512
    updated, rows = pl.pallas_call(
        project_kernel,
        grid=(2048 // nb,),
        out_shape=(sds((TOK, 2048), BF), sds((N_DEV * CAP, 16, HD), BF)),
        in_specs=[SM, full((4, TOK, 512)), pl.BlockSpec((2048, nb), lambda i: (0, i)),
                  pl.BlockSpec((TOK, nb), lambda i: (0, i)), full((1, 2048))],
        out_specs=(pl.BlockSpec((TOK, nb), lambda i: (0, i)), full((N_DEV * CAP, 16, HD))),
        scratch_shapes=[pltpu.VMEM((2048 // nb, TOK, nb), F32), pltpu.VMEM((TOK, 1), F32),
                        pltpu.VMEM((TOK, 16, HD), F32)],
        compiler_params=params(), name="project",
    )(slots, tok, weight, resid[0], norm_gain[None])

    def swap(a, cid, name):
        return pl.pallas_call(
            swap_kernel,
            out_shape=sds((N_DEV, CAP, 16, HD), BF),
            in_specs=[VM], out_specs=VM,
            scratch_shapes=[sem, sem],
            compiler_params=params(cid=cid), name=name,
        )(a.reshape(N_DEV, CAP, 16, HD)).reshape(N_DEV * CAP, 16, HD)

    came = swap(rows, 2, "dispatch")
    n = N_DEV * CAP
    answered = pl.pallas_call(
        expert_kernel,
        grid=(8,),
        out_shape=sds((n, 16, HD), BF),
        in_specs=[full((n, 16, HD)), pl.BlockSpec((2048, 256), lambda i: (0, jnp.minimum(i, 3))),
                  pl.BlockSpec((2048, 256), lambda i: (0, jnp.minimum(i, 3))),
                  pl.BlockSpec((1024, 512), lambda i: (0, jnp.maximum(i - 4, 0)))],
        out_specs=full((n, 16, HD)),
        scratch_shapes=[pltpu.VMEM((n, 16, HD), F32), pltpu.VMEM((n, 2048), BF), pltpu.VMEM((4, n, 256), BF)],
        compiler_params=params(), name="expert",
    )(came, expert_gate[0], expert_up[0], expert_down[0])
    returned = swap(answered, 3, "answers_back")
    out = pl.pallas_call(
        combine_kernel,
        out_shape=sds((TOK, 2048), BF),
        in_specs=[SM, SM, VM, VM], out_specs=VM,
        scratch_shapes=[pltpu.VMEM((TOK, 16, HD), F32)],
        compiler_params=params(), name="combine",
    )(target, route_weight[0].reshape(1, 2 * TOK), returned, updated)
    return out[None]


def solution(mesh):
    placed = (
        P("dp", "sp", None),
        P("dp", "sp", None),
        P("dp", "sp", None),
        P("dp", "sp", None),
        P(),
        P(),
        P("dp", None),
        P(),
        P("dp", "sp", None),
        P("dp", "sp", None),
        P(("sp", "dp"), None, None),
        P(("sp", "dp"), None, None),
        P(("sp", "dp"), None, None),
    )
    return jax.shard_map(
        per_device, mesh=mesh, in_specs=placed, out_specs=P("dp", "sp", None), check_vma=False
    )
```

```python
import functools
import jax
import jax.numpy as jnp
from jax import lax
from jax.experimental import pallas as pl
from jax.experimental.pallas import tpu as pltpu
from jax.sharding import PartitionSpec as P

GRID_W = 64
EPSILON = 1e-06
THETA = 10000.0
LIMIT = 7.0
SLOPE = 1.702
LOG2E = 1.4426950408889634
HD = 128
TOK = 256
ZN = 4
XN = 4
N_DEV = 128
CAP = 6
BF = jnp.bfloat16
F32 = jnp.float32
MESH = pl.DeviceIdType.MESH
VM = pl.BlockSpec(memory_space=pltpu.VMEM)
SM = pl.BlockSpec(memory_space=pltpu.SMEM)
MB = 1 << 20


def params(limit=48 * MB, cid=None, **kw):
    if cid is not None:
        kw.update(collective_id=cid, has_side_effects=True)
    return pltpu.CompilerParams(vmem_limit_bytes=limit, **kw)


def turn_tables(places):
    lane = jnp.arange(HD, dtype=jnp.int32)
    inverse = THETA ** (-(lane % 32).astype(F32) / 32)
    place = jnp.where(lane[None, :] < 64, (places // GRID_W)[:, None], (places % GRID_W)[:, None])
    angles = place.astype(F32) * inverse[None, :]
    sign = jnp.where(lane % 64 < 32, -1.0, 1.0)
    return jnp.cos(angles), jnp.sin(angles) * sign[None, :]


def turn_head(x, gain, cosine, sine, first):
    x = x.astype(F32)
    x = x * lax.rsqrt(jnp.mean(x * x, axis=-1, keepdims=True) + EPSILON) * gain
    other = jnp.where(first, pltpu.roll(x, HD - 32, 1), pltpu.roll(x, 32, 1))
    return (x * cosine + other * sine).astype(BF)


def prep_kernel(q_ref, k_ref, v_ref, qg_ref, kg_ref, cos_ref, sin_ref, idr_ref, idc_ref,
                qs_ref, kvs_ref, tgt_ref, slot_ref):
    first = lax.broadcasted_iota(jnp.int32, (TOK, HD), 1) % 64 < 32
    cosine, sine = cos_ref[...], sin_ref[...]
    for h in range(16):
        qs_ref[h // 4, :, (h % 4) * HD:(h % 4 + 1) * HD] = turn_head(
            q_ref[:, h * HD:(h + 1) * HD], qg_ref[...], cosine, sine, first)
    for h in range(4):
        kvs_ref[h, 0] = turn_head(k_ref[:, h * HD:(h + 1) * HD], kg_ref[...], cosine, sine, first)
        kvs_ref[h, 1] = v_ref[:, h * HD:(h + 1) * HD]
    n = 2 * TOK
    row, col = idr_ref[...], idc_ref[...]
    ia = lax.broadcasted_iota(jnp.int32, (n, n), 0)
    ib = lax.broadcasted_iota(jnp.int32, (n, n), 1)
    same = col == row
    before = jnp.sum(jnp.where(same & (ia < ib), 1.0, 0.0), axis=0, keepdims=True)
    tgt_ref[...] = row * CAP + before.astype(jnp.int32)
    before_c = jnp.sum(jnp.where(same & (ib < ia), 1.0, 0.0), axis=1, keepdims=True)
    target = col * CAP + before_c.astype(jnp.int32)
    slots = lax.broadcasted_iota(jnp.int32, (n, N_DEV * CAP), 1)
    token = (lax.broadcasted_iota(jnp.int32, (n, N_DEV * CAP), 0) // 2).astype(F32)
    slot_ref[...] = jnp.sum(jnp.where(target == slots, token, 0.0), axis=0, keepdims=True).astype(jnp.int32)


def sp_of(z, x):
    return {"sp": lax.rem(z, ZN) * XN + lax.rem(x, XN)}


def spread_kernel(qs_ref, kvs_ref, q_ref, kv_ref, zks, zkr, zqs, zqr, xs, xr, fs, fr):
    sp = lax.axis_index("sp")
    z, x = sp // XN, lax.rem(sp, XN)
    bar = pltpu.get_barrier_semaphore()
    for d in (1, 2, 3):
        pl.semaphore_signal(bar, inc=1, device_id=sp_of(z + d, x), device_id_type=MESH)
    for d in (1, 3):
        pl.semaphore_signal(bar, inc=1, device_id=sp_of(z, x + d), device_id_type=MESH)
    pl.semaphore_wait(bar, 5)
    pending = []

    def send(src, dst, ssem, rsem, dev):
        c = pltpu.make_async_remote_copy(src, dst, ssem, rsem, device_id=dev, device_id_type=MESH)
        c.start()
        pending.append(c)
        return c

    zk = {}
    for d in (1, 3, 2):
        zk[d] = send(kvs_ref.at[lax.rem(z + d, ZN)], kv_ref.at[x, z], zks.at[d - 1], zkr.at[d - 1], sp_of(z + d, x))
    kv_ref[x, z] = kvs_ref[z]

    def gather(d):
        chunk = lax.rem(z + ZN - d, ZN)
        return [send(kv_ref.at[x, chunk], kv_ref.at[x, chunk], xs.at[s, d], xr.at[s, d], sp_of(z, x + (1, 3)[s])) for s in (0, 1)]

    near = {0: gather(0)}
    zq = {}
    for d in (1, 3, 2):
        zq[d] = send(qs_ref.at[lax.rem(z + d, ZN)], q_ref.at[z], zqs.at[d - 1], zqr.at[d - 1], sp_of(z + d, x))
    q_ref[z] = qs_ref[z]
    far = []

    def forward(d):
        chunk = lax.rem(z + ZN - d, ZN)
        s = 0 if d in (0, 1) else 1
        near[d][s].wait_recv()
        came = lax.rem(x + (3, 1)[s], XN)
        far.append(send(kv_ref.at[came, chunk], kv_ref.at[came, chunk], fs.at[d], fr.at[d], sp_of(z, x + (1, 3)[s])))

    prev = 0
    for d in (1, 3, 2):
        zk[d].wait_recv()
        near[d] = gather(d)
        forward(prev)
        prev = d
    forward(prev)
    for d in (0, 1, 2, 3):
        s = 0 if d in (0, 1) else 1
        near[d][1 - s].wait_recv()
    for d in (1, 3, 2):
        zq[d].wait_recv()
    for c in far:
        c.wait_recv()
    for c in pending:
        c.wait_send()


def attend_kernel(q_ref, kv_ref, o_ref, ve_ref):
    scale = HD ** -0.5 * LOG2E

    @pl.when(pl.program_id(0) == 0)
    def _():
        lane = lax.broadcasted_iota(jnp.int32, (1024, HD), 1)
        for c in range(4):
            ve_ref[c * 1024:(c + 1) * 1024, :HD] = kv_ref[c, :, 1].reshape(1024, HD)
            ve_ref[c * 1024:(c + 1) * 1024, HD:] = jnp.where(lane == 0, 1.0, 0.0).astype(BF)

    q = q_ref[0]
    m = acc = None
    for c in range(4):
        k = kv_ref[c, :, 0].reshape(1024, HD)
        s = lax.dot_general(q, k, (((1,), (1,)), ((), ())), preferred_element_type=F32)
        top = jnp.max(s, axis=-1, keepdims=True) * scale
        m_new = top if m is None else jnp.maximum(m, top)
        p = jnp.exp2(s * scale - m_new).astype(BF)
        part = jnp.dot(p, ve_ref[c * 1024:(c + 1) * 1024, :], preferred_element_type=F32)
        acc = part if acc is None else acc * jnp.exp2(m - m_new) + part
        m = m_new
    o_ref[0] = (acc[:, :HD] / acc[:, HD:HD + 1]).astype(BF)


def gather_kernel(o_ref, r_ref, ss, rs):
    sp = lax.axis_index("sp")
    z, x = sp // XN, lax.rem(sp, XN)
    bar = pltpu.get_barrier_semaphore()
    for d in (1, 2, 3):
        pl.semaphore_signal(bar, inc=1, device_id=sp_of(z + d, x), device_id_type=MESH)
    pl.semaphore_wait(bar, 3)
    cs = []
    for d in (1, 3, 2):
        c = pltpu.make_async_remote_copy(o_ref.at[lax.rem(z + d, ZN)], r_ref.at[z], ss.at[d - 1], rs.at[d - 1],
                                         device_id=sp_of(z + d, x), device_id_type=MESH)
        c.start()
        cs.append(c)
    r_ref[z] = o_ref[z]
    for c in cs:
        c.wait()


def project_kernel(t_ref, w_ref, r_ref, g_ref, u_ref, out_ref, u2, sq, n3):
    i = pl.program_id(0)
    nb = w_ref.shape[1]
    y = r_ref[...].astype(F32)
    acc = jnp.dot(t_ref[0], w_ref[0:512, :], preferred_element_type=F32)
    for k in range(1, 4):
        acc = acc + jnp.dot(t_ref[k], w_ref[k * 512:(k + 1) * 512, :], preferred_element_type=F32)
    u = (y + acc).astype(BF)
    u_ref[...] = u
    wide = u.astype(F32)
    u2[i] = wide
    part = jnp.sum(wide * wide, axis=-1, keepdims=True)

    @pl.when(i == 0)
    def _():
        sq[...] = part

    @pl.when(i > 0)
    def _():
        sq[...] += part

    @pl.when(i == pl.num_programs(0) - 1)
    def _():
        inv = lax.rsqrt(sq[...] / 2048.0 + EPSILON)
        per = nb // HD
        for j in range(16):
            piece = u2[j // per, :, (j % per) * HD:(j % per + 1) * HD]
            n3[:, j, :] = (piece * inv * g_ref[:, j * HD:(j + 1) * HD]).astype(BF).astype(F32)

        def narrow(t, _):
            rows = pl.ds(t * 8, 8)
            out_ref[rows] = n3[rows].astype(BF)
            return 0

        lax.fori_loop(0, TOK // 8, narrow, 0)


GROUPS = 4
PER = N_DEV // GROUPS
STEP = 37


def moe_kernel(slot_ref, tgt_ref, wt_ref, n_ref, u_ref, wg_hbm, wu_hbm, wd_hbm, o_ref,
               wg, wu, wd, rows, came, y, ret, w3, xs, act, c3, wsem, ss, rs, ys, yr):
    me = lax.axis_index("sp") * 8 + lax.axis_index("dp")
    bar = pltpu.get_barrier_semaphore()
    n = PER * CAP

    def dev(p):
        return {"sp": p // 8, "dp": lax.rem(p, 8)}

    def ahead(i):
        return lax.rem(me + i * STEP, N_DEV)

    def behind(i):
        return lax.rem(me + i * (N_DEV - STEP), N_DEV)

    def sig(i, _):
        pl.semaphore_signal(bar, inc=1, device_id=dev(lax.rem(me + i, N_DEV)), device_id_type=MESH)
        return 0

    lax.fori_loop(1, N_DEV, sig, 0)
    loads = []
    for k in range(4):
        for src, dst in ((wg_hbm.at[:, k * 256:(k + 1) * 256], wg.at[k]), (wu_hbm.at[:, k * 256:(k + 1) * 256], wu.at[k]),
                         (wd_hbm.at[:, k * 512:(k + 1) * 512], wd.at[k])):
            c = pltpu.make_async_copy(src, dst, wsem.at[len(loads)])
            c.start()
            loads.append(c)

    def pick(i, _):
        p = ahead(i)
        for r in range(CAP):
            rows[i, r] = n_ref[slot_ref[0, p * CAP + r]]
        return 0

    def send(i, _):
        p = ahead(i)
        pltpu.make_async_remote_copy(rows.at[i], came.at[i], ss, rs.at[i // PER], device_id=dev(p), device_id_type=MESH).start()
        return 0

    lax.fori_loop(0, PER, pick, 0)
    came[0] = rows[0]
    pl.semaphore_wait(bar, N_DEV - 1)
    lax.fori_loop(1, PER, send, 0)
    for g in range(1, GROUPS):
        lax.fori_loop(g * PER, (g + 1) * PER, pick, 0)
        lax.fori_loop(g * PER, (g + 1) * PER, send, 0)
    for c in loads:
        c.wait()

    def group(g, _):
        base = g * PER

        def arrived(first, count, sem):
            part = pl.ds(first, count)
            pltpu.make_async_remote_copy(rows.at[part], came.at[part], ss, sem, device_id=dev(me), device_id_type=MESH).wait_recv()

        @pl.when(g == 0)
        def _():
            arrived(1, PER - 1, rs.at[0])

        @pl.when(g > 0)
        def _():
            arrived(base, PER, rs.at[g])

        def widen(t, _):
            for r in range(CAP):
                w3[t * CAP + r] = came[base + t, r].astype(F32)
            return 0

        lax.fori_loop(0, PER, widen, 0)
        for j in range(16):
            xs[:, j * HD:(j + 1) * HD] = w3[:, j, :].astype(BF)

        def up(k, _):
            x = xs[...]
            a = jnp.minimum(jnp.dot(x, wg[k], preferred_element_type=F32), LIMIT)
            b = jnp.clip(jnp.dot(x, wu[k], preferred_element_type=F32), -LIMIT, LIMIT)
            act[k] = (a * jax.nn.sigmoid(SLOPE * a) * (b + 1.0)).astype(BF)
            return 0

        lax.fori_loop(0, 4, up, 0)

        for k in range(4):
            d = jnp.dot(act[0], wd[k, 0:256, :], preferred_element_type=F32)
            for m in range(1, 4):
                d = d + jnp.dot(act[m], wd[k, m * 256:(m + 1) * 256, :], preferred_element_type=F32)
            for j in range(4):
                w3[:, k * 4 + j, :] = d[:, j * HD:(j + 1) * HD]

        def narrow(t, _):
            for r in range(CAP):
                y[base + t, r] = w3[t * CAP + r].astype(BF)
            return 0

        lax.fori_loop(0, PER, narrow, 0)

        def answer(t, _):
            i = base + t
            pltpu.make_async_remote_copy(y.at[i], ret.at[me], ys, yr, device_id=dev(behind(i)), device_id_type=MESH).start()
            return 0

        @pl.when(g == 0)
        def _():
            ret[me] = y[0]
            lax.fori_loop(1, PER, answer, 0)

        @pl.when(g > 0)
        def _():
            lax.fori_loop(0, PER, answer, 0)

        return 0

    lax.fori_loop(0, GROUPS, group, 0)
    rest = pl.ds(0, N_DEV - 1)
    pltpu.make_async_remote_copy(y.at[rest], ret.at[rest], ys, yr, device_id=dev(me), device_id_type=MESH).wait()
    pltpu.make_async_remote_copy(rows.at[rest], came.at[rest], ss, rs.at[0], device_id=dev(me), device_id_type=MESH).wait_send()

    def token(t, _):
        for h in range(4):
            q = t * 4 + h
            i0, i1 = tgt_ref[0, 2 * q], tgt_ref[0, 2 * q + 1]
            a = ret[i0 // CAP, lax.rem(i0, CAP)].astype(F32) * wt_ref[0, 2 * q]
            b = ret[i1 // CAP, lax.rem(i1, CAP)].astype(F32) * wt_ref[0, 2 * q + 1]
            c3[q] = a + b
        return 0

    lax.fori_loop(0, TOK // 4, token, 0)
    for j in range(16):
        cols = slice(j * HD, (j + 1) * HD)
        o_ref[:, cols] = (u_ref[:, cols].astype(F32) + c3[:, j, :]).astype(BF)


def full(shape):
    return pl.BlockSpec(shape, lambda *i: (0,) * len(shape))


def per_device(resid, query, keys, values, q_gain, k_gain, out_weight, norm_gain, route_ids, route_weight,
               expert_gate, expert_up, expert_down):
    sds = jax.ShapeDtypeStruct
    sem = pltpu.SemaphoreType.DMA
    weight = lax.all_gather(out_weight, "dp", axis=0, tiled=True)
    places = lax.axis_index("sp") * TOK + jnp.arange(TOK, dtype=jnp.int32)
    cosine, sine = turn_tables(places)
    ids = route_ids[0].reshape(1, 2 * TOK)
    qs, kvs, target, slots = pl.pallas_call(
        prep_kernel,
        out_shape=(sds((4, TOK, 512), BF), sds((4, 2, TOK, HD), BF), sds((1, 2 * TOK), jnp.int32),
                   sds((1, N_DEV * CAP), jnp.int32)),
        compiler_params=params(), name="prep",
    )(query[0], keys[0], values[0], q_gain[None], k_gain[None], cosine, sine, ids, ids.reshape(2 * TOK, 1))
    qr, kvr = pl.pallas_call(
        spread_kernel,
        out_shape=(sds((4, TOK, 512), BF), sds((4, 4, 2, TOK, HD), BF)),
        in_specs=[VM, VM], out_specs=(VM, VM),
        scratch_shapes=[sem((3,)), sem((3,)), sem((3,)), sem((3,)), sem((2, 4)), sem((2, 4)), sem((4,)), sem((4,))],
        compiler_params=params(cid=0), name="spread",
    )(qs, kvs)
    heads = pl.pallas_call(
        attend_kernel,
        grid=(16,),
        out_shape=sds((4, TOK, 512), BF),
        in_specs=[pl.BlockSpec((1, TOK, HD), lambda i: (i // 4, 0, i % 4)), full((4, 4, 2, TOK, HD))],
        out_specs=pl.BlockSpec((1, TOK, HD), lambda i: (i // 4, 0, i % 4)),
        scratch_shapes=[pltpu.VMEM((4096, 256), BF)],
        compiler_params=params(), name="attend",
        cost_estimate=pl.CostEstimate(flops=17_000_000_000, bytes_accessed=4_000_000, transcendentals=16_000_000),
    )(qr, kvr)
    tok = pl.pallas_call(
        gather_kernel,
        out_shape=sds((4, TOK, 512), BF),
        in_specs=[VM], out_specs=VM,
        scratch_shapes=[sem((3,)), sem((3,))],
        compiler_params=params(cid=1), name="heads_back",
    )(heads)
    nb = 512
    updated, rows = pl.pallas_call(
        project_kernel,
        grid=(2048 // nb,),
        out_shape=(sds((TOK, 2048), BF), sds((TOK, 16, HD), BF)),
        in_specs=[full((4, TOK, 512)), pl.BlockSpec((2048, nb), lambda i: (0, i)),
                  pl.BlockSpec((TOK, nb), lambda i: (0, i)), full((1, 2048))],
        out_specs=(pl.BlockSpec((TOK, nb), lambda i: (0, i)), full((TOK, 16, HD))),
        scratch_shapes=[pltpu.VMEM((2048 // nb, TOK, nb), F32), pltpu.VMEM((TOK, 1), F32),
                        pltpu.VMEM((TOK, 16, HD), F32)],
        compiler_params=params(), name="project",
    )(tok, weight, resid[0], norm_gain[None])

    tiles = pltpu.VMEM((N_DEV, CAP, 16, HD), BF)
    n = PER * CAP
    out = pl.pallas_call(
        moe_kernel,
        out_shape=sds((TOK, 2048), BF),
        in_specs=[SM, SM, SM, VM, VM] + [pl.BlockSpec(memory_space=pl.ANY)] * 3, out_specs=VM,
        scratch_shapes=[pltpu.VMEM((4, 2048, 256), BF), pltpu.VMEM((4, 2048, 256), BF), pltpu.VMEM((4, 1024, 512), BF),
                        tiles, tiles, tiles, tiles, pltpu.VMEM((n, 16, HD), F32), pltpu.VMEM((n, 2048), BF),
                        pltpu.VMEM((4, n, 256), BF), pltpu.VMEM((TOK, 16, HD), F32),
                        sem((12,)), sem, sem((GROUPS,)), sem, sem],
        compiler_params=params(cid=2), name="moe",
    )(slots, target, route_weight[0].reshape(1, 2 * TOK), rows, updated, expert_gate[0], expert_up[0], expert_down[0])
    return out[None]


def solution(mesh):
    placed = (
        P("dp", "sp", None),
        P("dp", "sp", None),
        P("dp", "sp", None),
        P("dp", "sp", None),
        P(),
        P(),
        P("dp", None),
        P(),
        P("dp", "sp", None),
        P("dp", "sp", None),
        P(("sp", "dp"), None, None),
        P(("sp", "dp"), None, None),
        P(("sp", "dp"), None, None),
    )
    return jax.shard_map(
        per_device, mesh=mesh, in_specs=placed, out_specs=P("dp", "sp", None), check_vma=False
    )
```

```python
import functools
import jax
import jax.numpy as jnp
from jax import lax
from jax.experimental import pallas as pl
from jax.experimental.pallas import tpu as pltpu
from jax.sharding import PartitionSpec as P

GRID_W = 64
EPSILON = 1e-06
THETA = 10000.0
LIMIT = 7.0
SLOPE = 1.702
LOG2E = 1.4426950408889634
HD = 128
TOK = 256
ZN = 4
XN = 4
N_DEV = 128
CAP = 6
BF = jnp.bfloat16
F32 = jnp.float32
MESH = pl.DeviceIdType.MESH
VM = pl.BlockSpec(memory_space=pltpu.VMEM)
SM = pl.BlockSpec(memory_space=pltpu.SMEM)
MB = 1 << 20


def params(limit=48 * MB, cid=None, **kw):
    if cid is not None:
        kw.update(collective_id=cid, has_side_effects=True)
    return pltpu.CompilerParams(vmem_limit_bytes=limit, **kw)


def turn_tables(places):
    lane = jnp.arange(HD, dtype=jnp.int32)
    inverse = THETA ** (-(lane % 32).astype(F32) / 32)
    place = jnp.where(lane[None, :] < 64, (places // GRID_W)[:, None], (places % GRID_W)[:, None])
    angles = place.astype(F32) * inverse[None, :]
    sign = jnp.where(lane % 64 < 32, -1.0, 1.0)
    return jnp.cos(angles), jnp.sin(angles) * sign[None, :]


def turn_head(x, gain, cosine, sine, first):
    x = x.astype(F32)
    x = x * lax.rsqrt(jnp.mean(x * x, axis=-1, keepdims=True) + EPSILON) * gain
    other = jnp.where(first, pltpu.roll(x, HD - 32, 1), pltpu.roll(x, 32, 1))
    return (x * cosine + other * sine).astype(BF)


def sp_of(z, x):
    return {"sp": lax.rem(z, ZN) * XN + lax.rem(x, XN)}


def dp_of(y, c):
    return lax.rem(y, 4) * 2 + lax.rem(c, 2)


def route_tables(ids_ref, tgt_ref, slot_ref):
    n = 2 * TOK
    row = ids_ref[...].astype(F32)
    ia = lax.broadcasted_iota(jnp.int32, (n, n), 0)
    ib = lax.broadcasted_iota(jnp.int32, (n, n), 1)
    col = jnp.sum(jnp.where(ia == ib, row, 0.0), axis=1, keepdims=True)
    same = col == row
    before = jnp.sum(jnp.where(same & (ia < ib), 1.0, 0.0), axis=0, keepdims=True)
    tgt_ref[...] = (row * CAP + before).astype(jnp.int32)
    before_c = jnp.sum(jnp.where(same & (ib < ia), 1.0, 0.0), axis=1, keepdims=True)
    target = (col * CAP + before_c).astype(jnp.int32)
    slots = lax.broadcasted_iota(jnp.int32, (n, N_DEV * CAP), 1)
    token = (lax.broadcasted_iota(jnp.int32, (n, N_DEV * CAP), 0) // 2).astype(F32)
    slot_ref[...] = jnp.sum(jnp.where(target == slots, token, 0.0), axis=0, keepdims=True).astype(jnp.int32)


def attend(q, kv_ref, ve_ref):
    scale = HD ** -0.5 * LOG2E
    q = jnp.concatenate([q[:, h * HD:(h + 1) * HD] for h in range(4)], axis=0)
    m = acc = None
    for c in range(8):
        k = kv_ref[c // 2, (c % 2) * 2:(c % 2) * 2 + 2, 0].reshape(512, HD)
        s = lax.dot_general(q, k, (((1,), (1,)), ((), ())), preferred_element_type=F32)
        top = jnp.max(s, axis=-1, keepdims=True) * scale
        m_new = top if m is None else jnp.maximum(m, top)
        p = jnp.exp2(s * scale - m_new).astype(BF)
        part = jnp.dot(p, ve_ref[c * 512:(c + 1) * 512, :], preferred_element_type=F32)
        acc = part if acc is None else acc * jnp.exp2(m - m_new) + part
        m = m_new
    return (acc[:, :HD] / acc[:, HD:HD + 1]).astype(BF)


def front_kernel(q_hbm, k_hbm, v_hbm, r_hbm, w_hbm, cos_hbm, sin_hbm, qg_ref, kg_ref, ng_ref, ids_ref,
                 u_ref, n_ref, tgt_ref, slot_ref,
                 qv, kx, vx, rv, wv, cosv, sinv, qs, kvs, qr, kvr, ve, heads, tok, n3,
                 ls, zks, zkr, zqs, zqr, xs, xr, fs, fr, hs, hr, w1s, w1r, w2s, w2r, wss, wsr):
    sp, dp = lax.axis_index("sp"), lax.axis_index("dp")
    z, x = sp // XN, lax.rem(sp, XN)
    yy, core = dp // 2, lax.rem(dp, 2)
    above, below, mate = dp_of(yy + 1, core), dp_of(yy + 3, core), dp_of(yy, core + 1)
    far_shard = dp_of(yy + 2, core)
    bar = pltpu.get_barrier_semaphore()
    for d in (1, 2, 3):
        pl.semaphore_signal(bar, inc=1, device_id=sp_of(z + d, x), device_id_type=MESH)
    for d in (1, 3):
        pl.semaphore_signal(bar, inc=1, device_id=sp_of(z, x + d), device_id_type=MESH)
    for p in (above, below, mate):
        pl.semaphore_signal(bar, inc=1, device_id={"dp": p}, device_id_type=MESH)
    loads = {}
    for i, (name, src, dst) in enumerate((("w", w_hbm, wv.at[dp]), ("k", k_hbm, kx), ("cos", cos_hbm, cosv), ("sin", sin_hbm, sinv),
                                          ("v", v_hbm, vx), ("q", q_hbm, qv), ("r", r_hbm, rv))):
        loads[name] = pltpu.make_async_copy(src, dst, ls.at[i])
        loads[name].start()
    pending = []

    def remote(src, dst, ssem, rsem, dev):
        return pltpu.make_async_remote_copy(src, dst, ssem, rsem, device_id=dev, device_id_type=MESH)

    def send(src, dst, ssem, rsem, dev):
        c = remote(src, dst, ssem, rsem, dev)
        c.start()
        pending.append(c)
        return c

    pl.semaphore_wait(bar, 8)
    loads["w"].wait()
    near_w = {}
    for half in (0, 1):
        for s, p in ((0, above), (1, below)):
            h = half if s == 0 else 1 - half
            near_w[s, h] = send(wv.at[dp, h], wv.at[dp, h], w1s.at[s, h], w1r.at[s, h], {"dp": p})
    mates = [send(wv.at[dp], wv.at[dp], wss.at[0], wsr.at[0], {"dp": mate})]

    first = lax.broadcasted_iota(jnp.int32, (TOK, HD), 1) % 64 < 32
    for name in ("k", "cos", "sin", "v"):
        loads[name].wait()
    cosine, sine = cosv[...], sinv[...]
    zk = {}
    for h in range(4):
        kvs[h, 0] = turn_head(kx[:, h * HD:(h + 1) * HD], kg_ref[...], cosine, sine, first)
        kvs[h, 1] = vx[:, h * HD:(h + 1) * HD]
    for d in (1, 3, 2):
        zk[d] = send(kvs.at[lax.rem(z + d, ZN)], kvr.at[x, z], zks.at[d - 1], zkr.at[d - 1], sp_of(z + d, x))
    kvr[x, z] = kvs[z]

    def gather(d):
        chunk = lax.rem(z + ZN - d, ZN)
        return [send(kvr.at[x, chunk], kvr.at[x, chunk], xs.at[s, d], xr.at[s, d], sp_of(z, x + (1, 3)[s])) for s in (0, 1)]

    loads["q"].wait()

    def turn_query(d):
        zz = lax.rem(z + d, ZN)
        for h in range(4):
            cols = pl.ds(pl.multiple_of(zz * 512 + h * HD, HD), HD)
            val = turn_head(qv[:, cols], qg_ref[...], cosine, sine, first)
            if d:
                qs[zz, :, h * HD:(h + 1) * HD] = val
            else:
                qr[zz, :, h * HD:(h + 1) * HD] = val
        return zz

    near = {0: gather(0)}
    for d in (3, 2, 1):
        zz = turn_query(d)
        send(qs.at[zz], qr.at[z], zqs.at[d - 1], zqr.at[d - 1], sp_of(z + d, x))
    far = []

    def forward(d):
        chunk = lax.rem(z + ZN - d, ZN)
        s = 0 if d in (0, 1) else 1
        near[d][s].wait_recv()
        came = lax.rem(x + (3, 1)[s], XN)
        far.append(send(kvr.at[came, chunk], kvr.at[came, chunk], fs.at[d], fr.at[d], sp_of(z, x + (1, 3)[s])))

    zk[1].wait_recv()
    near[1] = gather(1)
    turn_query(0)
    forward(0)
    zk[3].wait_recv()
    near[3] = gather(3)
    zk[2].wait_recv()
    near[2] = gather(2)
    route_tables(ids_ref, tgt_ref, slot_ref)
    forward(1)
    near_w[0, 0].wait_recv()
    far_w = [send(wv.at[below, 0], wv.at[below, 0], w2s.at[0], w2r.at[0], {"dp": above})]
    near_w[1, 1].wait_recv()
    far_w.append(send(wv.at[above, 1], wv.at[above, 1], w2s.at[1], w2r.at[1], {"dp": below}))
    forward(3)
    forward(2)
    for d in (0, 1, 2, 3):
        s = 0 if d in (0, 1) else 1
        near[d][1 - s].wait_recv()
    for c in far:
        c.wait_recv()
    lane = lax.broadcasted_iota(jnp.int32, (1024, HD), 1)
    for c in range(4):
        ve[c * 1024:(c + 1) * 1024, :HD] = kvr[c, :, 1].reshape(1024, HD)
        ve[c * 1024:(c + 1) * 1024, HD:] = jnp.where(lane == 0, 1.0, 0.0).astype(BF)

    def block(t, _):
        a = lax.rem(z + 1 + t, ZN)

        @pl.when(t < 3)
        def _():
            remote(qs.at[a], qr.at[a], zqs.at[2 - t], zqr.at[2 - t], sp_of(a, x)).wait_recv()

        o = attend(qr[a], kvr, ve)
        for h in range(4):
            heads[a, :, h * HD:(h + 1) * HD] = o[h * TOK:(h + 1) * TOK]

        @pl.when(t < 3)
        def _():
            remote(heads.at[a], tok.at[z], hs.at[t], hr.at[t], sp_of(a, x)).start()

        @pl.when(t == 0)
        def _():
            near_w[0, 1].wait_recv()
            remote(wv.at[below], wv.at[below], wss.at[1], wsr.at[1], {"dp": mate}).start()
            near_w[1, 0].wait_recv()
            remote(wv.at[above], wv.at[above], wss.at[2], wsr.at[2], {"dp": mate}).start()

        @pl.when(t == 2)
        def _():
            for c in far_w:
                c.wait_recv()
            remote(wv.at[far_shard], wv.at[far_shard], wss.at[3], wsr.at[3], {"dp": mate}).start()

        return 0

    lax.fori_loop(0, 4, block, 0)
    tok[z] = heads[z]
    for i in range(1, 4):
        c = remote(wv.at[dp], wv.at[dp], wss.at[i], wsr.at[i], {"dp": mate})
        pending.append(c)
        c.wait_recv()
    mates[0].wait_recv()
    loads["r"].wait()
    for t in range(3):
        c = remote(heads.at[t], tok.at[t], hs.at[t], hr.at[t], sp_of(z + 1, x))
        pending.append(c)
        c.wait_recv()
    for c in pending:
        c.wait_send()

    sq = None
    for nb in range(4):
        cols = slice(nb * 512, (nb + 1) * 512)
        acc = None
        for k in range(4):
            w = wv[2 * k:2 * k + 2, :, :, cols].reshape(512, 512)
            part = jnp.dot(tok[k], w, preferred_element_type=F32)
            acc = part if acc is None else acc + part
        u = (rv[:, cols].astype(F32) + acc).astype(BF)
        u_ref[:, cols] = u
        wide = u.astype(F32)
        part = jnp.sum(wide * wide, axis=-1, keepdims=True)
        sq = part if sq is None else sq + part
    inv = lax.rsqrt(sq / 2048.0 + EPSILON)
    for j in range(16):
        cols = slice(j * HD, (j + 1) * HD)
        n3[:, j, :] = u_ref[:, cols].astype(F32) * inv * ng_ref[:, cols]

    def narrow(t, _):
        rows = pl.ds(t * 8, 8)
        n_ref[rows] = n3[rows].astype(BF)
        return 0

    lax.fori_loop(0, TOK // 8, narrow, 0)


GROUPS = 4
PER = N_DEV // GROUPS
STEP = 37


def moe_kernel(slot_ref, tgt_ref, wt_ref, n_ref, u_ref, wg_hbm, wu_hbm, wd_hbm, o_ref,
               wg, wu, wd, rows, came, y, ret, w3, xs, act, c3, wsem, ss, rs, ys, yr):
    me = lax.axis_index("sp") * 8 + lax.axis_index("dp")
    bar = pltpu.get_barrier_semaphore()
    n = PER * CAP

    def dev(p):
        return {"sp": p // 8, "dp": lax.rem(p, 8)}

    def ahead(i):
        return lax.rem(me + i * STEP, N_DEV)

    def behind(i):
        return lax.rem(me + i * (N_DEV - STEP), N_DEV)

    def sig(i, _):
        pl.semaphore_signal(bar, inc=1, device_id=dev(lax.rem(me + i, N_DEV)), device_id_type=MESH)
        return 0

    lax.fori_loop(1, N_DEV, sig, 0)
    loads = []
    for k in range(4):
        for src, dst in ((wg_hbm.at[:, k * 256:(k + 1) * 256], wg.at[k]), (wu_hbm.at[:, k * 256:(k + 1) * 256], wu.at[k]),
                         (wd_hbm.at[:, k * 512:(k + 1) * 512], wd.at[k])):
            c = pltpu.make_async_copy(src, dst, wsem.at[len(loads)])
            c.start()
            loads.append(c)

    def pick(i, _):
        p = ahead(i)
        for r in range(CAP):
            rows[i, r] = n_ref[slot_ref[0, p * CAP + r]]
        return 0

    def send(i, _):
        p = ahead(i)
        pltpu.make_async_remote_copy(rows.at[i], came.at[i], ss, rs.at[i // PER], device_id=dev(p), device_id_type=MESH).start()
        return 0

    lax.fori_loop(0, PER, pick, 0)
    came[0] = rows[0]
    pl.semaphore_wait(bar, N_DEV - 1)
    lax.fori_loop(1, PER, send, 0)
    for g in range(1, GROUPS):
        lax.fori_loop(g * PER, (g + 1) * PER, pick, 0)
        lax.fori_loop(g * PER, (g + 1) * PER, send, 0)
    for c in loads:
        c.wait()

    def group(g, _):
        base = g * PER

        def arrived(first, count, sem):
            part = pl.ds(first, count)
            pltpu.make_async_remote_copy(rows.at[part], came.at[part], ss, sem, device_id=dev(me), device_id_type=MESH).wait_recv()

        @pl.when(g == 0)
        def _():
            arrived(1, PER - 1, rs.at[0])

        @pl.when(g > 0)
        def _():
            arrived(base, PER, rs.at[g])

        def widen(t, _):
            for r in range(CAP):
                w3[t * CAP + r] = came[base + t, r].astype(F32)
            return 0

        lax.fori_loop(0, PER, widen, 0)
        for j in range(16):
            xs[:, j * HD:(j + 1) * HD] = w3[:, j, :].astype(BF)

        def up(k, _):
            x = xs[...]
            a = jnp.minimum(jnp.dot(x, wg[k], preferred_element_type=F32), LIMIT)
            b = jnp.clip(jnp.dot(x, wu[k], preferred_element_type=F32), -LIMIT, LIMIT)
            act[k] = (a * jax.nn.sigmoid(SLOPE * a) * (b + 1.0)).astype(BF)
            return 0

        lax.fori_loop(0, 4, up, 0)

        for k in range(4):
            d = jnp.dot(act[0], wd[k, 0:256, :], preferred_element_type=F32)
            for m in range(1, 4):
                d = d + jnp.dot(act[m], wd[k, m * 256:(m + 1) * 256, :], preferred_element_type=F32)
            for j in range(4):
                w3[:, k * 4 + j, :] = d[:, j * HD:(j + 1) * HD]

        def narrow(t, _):
            for r in range(CAP):
                y[base + t, r] = w3[t * CAP + r].astype(BF)
            return 0

        lax.fori_loop(0, PER, narrow, 0)

        def answer(t, _):
            i = base + t
            pltpu.make_async_remote_copy(y.at[i], ret.at[me], ys, yr, device_id=dev(behind(i)), device_id_type=MESH).start()
            return 0

        @pl.when(g == 0)
        def _():
            ret[me] = y[0]
            lax.fori_loop(1, PER, answer, 0)

        @pl.when(g > 0)
        def _():
            lax.fori_loop(0, PER, answer, 0)

        return 0

    lax.fori_loop(0, GROUPS, group, 0)
    rest = pl.ds(0, N_DEV - 1)
    pltpu.make_async_remote_copy(y.at[rest], ret.at[rest], ys, yr, device_id=dev(me), device_id_type=MESH).wait()
    pltpu.make_async_remote_copy(rows.at[rest], came.at[rest], ss, rs.at[0], device_id=dev(me), device_id_type=MESH).wait_send()

    def token(t, _):
        for h in range(4):
            q = t * 4 + h
            i0, i1 = tgt_ref[0, 2 * q], tgt_ref[0, 2 * q + 1]
            a = ret[i0 // CAP, lax.rem(i0, CAP)].astype(F32) * wt_ref[0, 2 * q]
            b = ret[i1 // CAP, lax.rem(i1, CAP)].astype(F32) * wt_ref[0, 2 * q + 1]
            c3[q] = a + b
        return 0

    lax.fori_loop(0, TOK // 4, token, 0)
    for j in range(16):
        cols = slice(j * HD, (j + 1) * HD)
        o_ref[:, cols] = (u_ref[:, cols].astype(F32) + c3[:, j, :]).astype(BF)


def full(shape):
    return pl.BlockSpec(shape, lambda *i: (0,) * len(shape))


def per_device(resid, query, keys, values, q_gain, k_gain, out_weight, norm_gain, route_ids, route_weight,
               expert_gate, expert_up, expert_down):
    sds = jax.ShapeDtypeStruct
    sem = pltpu.SemaphoreType.DMA
    places = lax.axis_index("sp") * TOK + jnp.arange(TOK, dtype=jnp.int32)
    cosine, sine = turn_tables(places)
    ANY = pl.BlockSpec(memory_space=pl.ANY)
    V = pltpu.VMEM
    updated, rows, target, slots = pl.pallas_call(
        front_kernel,
        out_shape=(sds((TOK, 2048), BF), sds((TOK, 16, HD), BF), sds((1, 2 * TOK), jnp.int32),
                   sds((1, N_DEV * CAP), jnp.int32)),
        in_specs=[ANY] * 7 + [VM] * 4, out_specs=(VM,) * 4,
        scratch_shapes=[V((TOK, 2048), BF), V((TOK, 512), BF), V((TOK, 512), BF), V((TOK, 2048), BF),
                        V((8, 2, 128, 2048), BF), V((TOK, HD), F32), V((TOK, HD), F32),
                        V((4, TOK, 512), BF), V((4, 2, TOK, HD), BF), V((4, TOK, 512), BF), V((4, 4, 2, TOK, HD), BF),
                        V((4096, 256), BF), V((4, TOK, 512), BF), V((4, TOK, 512), BF), V((TOK, 16, HD), F32),
                        sem((7,)), sem((3,)), sem((3,)), sem((3,)), sem((3,)), sem((2, 4)), sem((2, 4)), sem((4,)), sem((4,)),
                        sem((3,)), sem((3,)), sem((2, 2)), sem((2, 2)), sem((2,)), sem((2,)), sem((4,)), sem((4,))],
        compiler_params=params(56 * MB, cid=0), name="front",
    )(query[0], keys[0], values[0], resid[0], out_weight.reshape(2, 128, 2048), cosine, sine,
      q_gain[None], k_gain[None], norm_gain[None], route_ids[0].reshape(1, 2 * TOK))
    tiles = pltpu.VMEM((N_DEV, CAP, 16, HD), BF)
    n = PER * CAP
    out = pl.pallas_call(
        moe_kernel,
        out_shape=sds((TOK, 2048), BF),
        in_specs=[SM, SM, SM, VM, VM] + [pl.BlockSpec(memory_space=pl.ANY)] * 3, out_specs=VM,
        scratch_shapes=[pltpu.VMEM((4, 2048, 256), BF), pltpu.VMEM((4, 2048, 256), BF), pltpu.VMEM((4, 1024, 512), BF),
                        tiles, tiles, tiles, tiles, pltpu.VMEM((n, 16, HD), F32), pltpu.VMEM((n, 2048), BF),
                        pltpu.VMEM((4, n, 256), BF), pltpu.VMEM((TOK, 16, HD), F32),
                        sem((12,)), sem, sem((GROUPS,)), sem, sem],
        compiler_params=params(cid=1), name="moe",
    )(slots, target, route_weight[0].reshape(1, 2 * TOK), rows, updated, expert_gate[0], expert_up[0], expert_down[0])
    return out[None]


def solution(mesh):
    placed = (
        P("dp", "sp", None),
        P("dp", "sp", None),
        P("dp", "sp", None),
        P("dp", "sp", None),
        P(),
        P(),
        P("dp", None),
        P(),
        P("dp", "sp", None),
        P("dp", "sp", None),
        P(("sp", "dp"), None, None),
        P(("sp", "dp"), None, None),
        P(("sp", "dp"), None, None),
    )
    return jax.shard_map(
        per_device, mesh=mesh, in_specs=placed, out_specs=P("dp", "sp", None), check_vma=False
    )
```

```python
import functools
import jax
import jax.numpy as jnp
from jax import lax
from jax.experimental import pallas as pl
from jax.experimental.pallas import tpu as pltpu
from jax.sharding import PartitionSpec as P

GRID_W = 64
EPSILON = 1e-06
THETA = 10000.0
LIMIT = 7.0
SLOPE = 1.702
LOG2E = 1.4426950408889634
HD = 128
TOK = 256
ZN = 4
XN = 4
N_DEV = 128
GROUPS = 4
PER = N_DEV // GROUPS
STEP = 37
CAP = 6
BF = jnp.bfloat16
F32 = jnp.float32
MESH = pl.DeviceIdType.MESH
VM = pl.BlockSpec(memory_space=pltpu.VMEM)
SM = pl.BlockSpec(memory_space=pltpu.SMEM)
MB = 1 << 20
LIM = 56


def params(limit=48 * MB, cid=None, **kw):
    if cid is not None:
        kw.update(collective_id=cid, has_side_effects=True)
    return pltpu.CompilerParams(vmem_limit_bytes=limit, **kw)


def turn_tables(sp):
    lane = jnp.arange(HD, dtype=jnp.int32)
    inverse = THETA ** (-(lane % 32).astype(F32) / 32)
    at = jnp.arange(GRID_W + 8, dtype=jnp.int32)
    place = jnp.where(at < GRID_W, at, sp * (TOK // GRID_W) + at - GRID_W)
    angles = place.astype(F32)[:, None] * inverse[None, :]
    sign = jnp.where(lane % 64 < 32, -1.0, 1.0)
    return jnp.cos(angles), jnp.sin(angles) * sign[None, :]


def per_token(table):
    lane = lax.broadcasted_iota(jnp.int32, (GRID_W, HD), 1)
    return jnp.concatenate(
        [jnp.where(lane < 64, table[GRID_W + b:GRID_W + b + 1, :], table[:GRID_W, :]) for b in range(TOK // GRID_W)], axis=0)


def turn_head(x, gain, cosine, sine, first):
    x = x.astype(F32)
    x = x * lax.rsqrt(jnp.mean(x * x, axis=-1, keepdims=True) + EPSILON) * gain
    other = jnp.where(first, pltpu.roll(x, HD - 32, 1), pltpu.roll(x, 32, 1))
    return (x * cosine + other * sine).astype(BF)


def sp_of(z, x):
    return {"sp": lax.rem(z, ZN) * XN + lax.rem(x, XN)}


def dp_of(y, c):
    return lax.rem(y, 4) * 2 + lax.rem(c, 2)


def route_tables(ids_ref, tgt_ref, slot_ref):
    n = 2 * TOK
    row = jnp.concatenate([ids_ref[0:1, :], ids_ref[1:2, :]], axis=1).astype(F32)
    ia = lax.broadcasted_iota(jnp.int32, (n, n), 0)
    ib = lax.broadcasted_iota(jnp.int32, (n, n), 1)
    col = jnp.sum(jnp.where(ia == ib, row, 0.0), axis=1, keepdims=True)
    same = col == row
    before = jnp.sum(jnp.where(same & (ia < ib), 1.0, 0.0), axis=0, keepdims=True)
    tgt_ref[...] = (row * CAP + before).astype(jnp.int32)
    before_c = jnp.sum(jnp.where(same & (ib < ia), 1.0, 0.0), axis=1, keepdims=True)
    target = (col * CAP + before_c).astype(jnp.int32)
    slots = lax.broadcasted_iota(jnp.int32, (n, N_DEV * CAP), 1)
    token = (lax.broadcasted_iota(jnp.int32, (n, N_DEV * CAP), 0) % TOK).astype(F32)
    slot_ref[...] = jnp.sum(jnp.where(target == slots, token, 0.0), axis=0, keepdims=True).astype(jnp.int32)


STEP_BLOCK = (3, 0, 1, 2, 0, 0, 1, 1, 0, 1, 2, 2, 2, 3, 3, 3)
STEP_QUARTER = (0, 0, 0, 0, 1, 3, 1, 3, 2, 2, 1, 3, 2, 1, 3, 2)


def step_entry(table, i):
    return sum(v * ((16 - lax.rem(i + 16 - k, 16)) // 16) for k, v in enumerate(table) if v)


def attend(q, kvr, ve, quarter, acc_ref, top_ref):
    scale = HD ** -0.5 * LOG2E
    q = jnp.concatenate([q[:, h * HD:(h + 1) * HD] for h in range(4)], axis=0)
    m, acc = jnp.max(top_ref[...], axis=-1, keepdims=True), acc_ref[...]
    for c in range(4):
        k = kvr[quarter, c, 0]
        s = lax.dot_general(q, k, (((1,), (1,)), ((), ())), preferred_element_type=F32)
        m_new = jnp.maximum(m, jnp.max(s, axis=-1, keepdims=True) * scale)
        p = jnp.exp2(s * scale - m_new).astype(BF)
        acc = acc * jnp.exp2(m - m_new) + jnp.dot(p, ve[quarter, c * TOK:(c + 1) * TOK, :], preferred_element_type=F32)
        m = m_new
    acc_ref[...] = acc
    top_ref[...] = jnp.broadcast_to(m, top_ref.shape)


def layer_kernel(q_hbm, k_hbm, v_hbm, r_hbm, w_hbm, wg_hbm, wu_hbm, wd_hbm, cos_ref, sin_ref, qg_ref, kg_ref, ng_ref, ids_ref, wt_ref,
                 o_ref,
                 qv, kx, vx, rv, wv, qs, kvs, qr, kvr, ve, heads, tok, n3, acc, tops, tgt_v, slot_v, tgt_s, slot_s,
                 u_ref, n_ref, wd, rows, came, ret, w3, xs_v, act,
                 ls, tsem, zks, zkr, zqs, zqr, xs, xr, fs, fr, hs, hr, w1s, w1r, w2s, w2r, wss, wsr, wsem, ss, rs, ys, yr, in_x, in_dp):
    sp, dp = lax.axis_index("sp"), lax.axis_index("dp")
    z, x = sp // XN, lax.rem(sp, XN)
    yy, core = dp // 2, lax.rem(dp, 2)
    me = sp * 8 + dp
    above, below, mate = dp_of(yy + 1, core), dp_of(yy + 3, core), dp_of(yy, core + 1)
    far_shard = dp_of(yy + 2, core)
    bar = pltpu.get_barrier_semaphore()

    def dev(p):
        return {"sp": p // 8, "dp": lax.rem(p, 8)}

    loads = {}
    for i, (name, src, dst) in enumerate((("k", k_hbm, kx), ("v", v_hbm, vx), ("q", q_hbm, qv), ("r", r_hbm, rv))):
        loads[name] = pltpu.make_async_copy(src, dst, ls.at[i])
        loads[name].start()

    w_loads = [pltpu.make_async_copy(w_hbm.at[:, nb * 512:(nb + 1) * 512], wv.at[nb, pl.ds(pl.multiple_of(dp * 256, 256), 256), :], ls.at[4 + nb])
               for nb in range(4)]
    for c in w_loads:
        c.start()

    def shard(p, half=None):
        if half is None:
            return wv.at[:, pl.ds(pl.multiple_of(p * 256, 256), 256), :]
        return wv.at[:, pl.ds(pl.multiple_of(p * 256 + half * 128, 128), 128), :]

    for d in (1, 2, 3):
        pl.semaphore_signal(bar, inc=1, device_id=sp_of(z + d, x), device_id_type=MESH)
        pl.semaphore_signal(bar, inc=1, device_id=sp_of(z, x + d), device_id_type=MESH)
    for d in range(1, 8):
        pl.semaphore_signal(bar, inc=1, device_id={"dp": lax.rem(dp + d, 8)}, device_id_type=MESH)
    weights = []
    for k in range(4):
        for src, dst in ((wg_hbm.at[:, k * 256:(k + 1) * 256], wv.at[k, :, 0:256]), (wu_hbm.at[:, k * 256:(k + 1) * 256], wv.at[k, :, 256:512]),
                         (wd_hbm.at[:, k * 512:(k + 1) * 512], wd.at[k])):
            weights.append(pltpu.make_async_copy(src, dst, wsem.at[len(weights)]))
    pending = []

    def remote(src, dst, ssem, rsem, dev):
        return pltpu.make_async_remote_copy(src, dst, ssem, rsem, device_id=dev, device_id_type=MESH)

    def send(src, dst, ssem, rsem, dev):
        c = remote(src, dst, ssem, rsem, dev)
        c.start()
        pending.append(c)
        return c

    pl.semaphore_wait(bar, 13)
    for d in (1, 2, 3):
        pl.semaphore_signal(in_x, inc=1, device_id=sp_of(z, x + d), device_id_type=MESH)
    for c in w_loads:
        c.wait()
    near_w = {}
    for half in (0, 1):
        for s, p in ((0, above), (1, below)):
            h = half if s == 0 else 1 - half
            near_w[s, h] = send(shard(dp, h), shard(dp, h), w1s.at[s, h], w1r.at[s, h], {"dp": p})
    mates = [send(shard(dp), shard(dp), wss.at[0], wsr.at[0], {"dp": mate})]
    first = lax.broadcasted_iota(jnp.int32, (TOK, HD), 1) % 64 < 32
    cosine, sine = per_token(cos_ref[...]), per_token(sin_ref[...])
    loads["k"].wait()
    loads["v"].wait()
    for h in range(4):
        kvs[h, 0] = turn_head(kx[:, h * HD:(h + 1) * HD], kg_ref[...], cosine, sine, first)
        kvs[h, 1] = vx[:, h * HD:(h + 1) * HD]
    zk = {}
    for d in (1, 3, 2):
        zk[d] = send(kvs.at[lax.rem(z + d, ZN)], kvr.at[x, z], zks.at[d - 1], zkr.at[d - 1], sp_of(z + d, x))
    kvr[x, z] = kvs[z]

    def gather(d):
        chunk = lax.rem(z + ZN - d, ZN)
        return [send(kvr.at[x, chunk], kvr.at[x, chunk], xs.at[s, d], xr.at[s, d], sp_of(z, x + (1, 3)[s])) for s in (0, 1)]

    near = {0: gather(0)}
    loads["q"].wait()

    def turn_query(d):
        zz = lax.rem(z + d, ZN)
        for h in range(4):
            cols = pl.ds(pl.multiple_of(zz * 512 + h * HD, HD), HD)
            val = turn_head(qv[:, cols], qg_ref[...], cosine, sine, first)
            if d:
                qs[zz, :, h * HD:(h + 1) * HD] = val
            else:
                qr[zz, :, h * HD:(h + 1) * HD] = val
        return zz

    for d in (3, 2, 1):
        zz = turn_query(d)
        send(qs.at[zz], qr.at[z], zqs.at[d - 1], zqr.at[d - 1], sp_of(z + d, x))
    def far_copy(d):
        chunk = lax.rem(z + ZN - d, ZN)
        s = 0 if d in (0, 1) else 1
        came_x = lax.rem(x + (3, 1)[s], XN)
        return remote(kvr.at[came_x, chunk], kvr.at[came_x, chunk], fs.at[d], fr.at[d], sp_of(z, x + (1, 3)[s]))

    def forward(d):
        near[d][0 if d in (0, 1) else 1].wait_recv()
        far_copy(d).start()

    far_w = [remote(shard(below, 0), shard(below, 0), w2s.at[0], w2r.at[0], {"dp": above}),
             remote(shard(above, 1), shard(above, 1), w2s.at[1], w2r.at[1], {"dp": below})]
    for c in weights[2::3]:
        c.start()
    route_tables(ids_ref, tgt_v, slot_v)
    tables = [pltpu.make_async_copy(tgt_v, tgt_s, tsem.at[0]), pltpu.make_async_copy(slot_v, slot_s, tsem.at[1])]
    for c in tables:
        c.start()
    pending += far_w + [far_copy(d) for d in range(4)]
    turn_query(0)
    pl.semaphore_wait(in_x, 3)
    for d in range(1, 8):
        pl.semaphore_signal(in_dp, inc=1, device_id={"dp": lax.rem(dp + d, 8)}, device_id_type=MESH)
    zk[1].wait_recv()
    near[1] = gather(1)
    zk[3].wait_recv()
    near[3] = gather(3)
    acc[...] = jnp.zeros_like(acc)
    tops[...] = jnp.full_like(tops, -jnp.inf)
    lane = lax.broadcasted_iota(jnp.int32, (1024, HD), 1)
    for c in range(4):
        ve[c, :, HD:] = jnp.where(lane == 0, 1.0, 0.0).astype(BF)
    zk[2].wait_recv()
    near[2] = gather(2)
    forward(0)

    def value_quarter(quarter):
        ve[quarter, :, :HD] = kvr[quarter, :, 1].reshape(1024, HD)

    value_quarter(x)

    def step(i, _):
        t, turn = step_entry(STEP_BLOCK, i), step_entry(STEP_QUARTER, i)
        a, quarter = lax.rem(z + 1 + t, ZN), lax.rem(x + ZN - turn, XN)

        @pl.when((i > 0) & (i < 4))
        def _():
            remote(qs.at[a], qr.at[a], zqs.at[2 - t], zqr.at[2 - t], sp_of(a, x)).wait_recv()

        @pl.when(i == 1)
        def _():
            forward(1)

        @pl.when(i == 3)
        def _():
            forward(3)

        @pl.when(i == 4)
        def _():
            forward(2)
            near[2][0].wait_recv()
            near[3][0].wait_recv()
            value_quarter(quarter)

        @pl.when(i == 5)
        def _():
            near[0][1].wait_recv()
            near[1][1].wait_recv()
            value_quarter(quarter)

        @pl.when(i == 6)
        def _():
            near_w[0, 0].wait_recv()
            remote(shard(below, 0), shard(below, 0), w2s.at[0], w2r.at[0], {"dp": above}).start()
            near_w[1, 1].wait_recv()
            remote(shard(above, 1), shard(above, 1), w2s.at[1], w2r.at[1], {"dp": below}).start()

        @pl.when(i == 8)
        def _():
            for d in range(4):
                far_copy(d).wait_recv()
            value_quarter(quarter)

        attend(qr[a], kvr, ve, quarter, acc.at[t], tops.at[t])

        @pl.when(turn == 2)
        def _():
            done = acc[t]
            out = (done[:, :HD] / done[:, HD:HD + 1]).astype(BF)
            for h in range(4):
                heads[a, :, h * HD:(h + 1) * HD] = out[h * TOK:(h + 1) * TOK]

        @pl.when((turn == 2) & (t < 3))
        def _():
            remote(heads.at[a], tok.at[z], hs.at[t], hr.at[t], sp_of(a, x)).start()

        @pl.when(i == 11)
        def _():
            near_w[0, 1].wait_recv()
            remote(shard(below), shard(below), wss.at[1], wsr.at[1], {"dp": mate}).start()
            near_w[1, 0].wait_recv()
            remote(shard(above), shard(above), wss.at[2], wsr.at[2], {"dp": mate}).start()

        return 0

    lax.fori_loop(0, 16, step, 0)
    for c in far_w:
        c.wait_recv()
    remote(shard(far_shard), shard(far_shard), wss.at[3], wsr.at[3], {"dp": mate}).start()
    tok[z] = heads[z]
    for i in range(1, 4):
        c = remote(shard(dp), shard(dp), wss.at[i], wsr.at[i], {"dp": mate})
        pending.append(c)
        c.wait_recv()
    mates[0].wait_recv()
    loads["r"].wait()
    for t in range(3):
        c = remote(heads.at[t], tok.at[t], hs.at[t], hr.at[t], sp_of(z + 1, x))
        pending.append(c)
        c.wait_recv()
    for c in pending:
        c.wait_send()

    sq = None
    for nb in range(4):
        cols = slice(nb * 512, (nb + 1) * 512)
        acc = None
        for k in range(4):
            part = jnp.dot(tok[k], wv[nb, k * 512:(k + 1) * 512, :], preferred_element_type=F32)
            acc = part if acc is None else acc + part
        u = (rv[:, cols].astype(F32) + acc).astype(BF)
        u_ref[:, cols] = u
        wide = u.astype(F32)
        part = jnp.sum(wide * wide, axis=-1, keepdims=True)
        sq = part if sq is None else sq + part
    for i, c in enumerate(weights):
        if i % 3 < 2:
            c.start()
    inv = lax.rsqrt(sq / 2048.0 + EPSILON)
    for j in range(16):
        cols = slice(j * HD, (j + 1) * HD)
        n3[:, j, :] = u_ref[:, cols].astype(F32) * inv * ng_ref[:, cols]

    def narrow(t, _):
        rows = pl.ds(t * 8, 8)
        n_ref[rows] = n3[rows].astype(BF)
        return 0

    lax.fori_loop(0, TOK // 8, narrow, 0)

    n = PER * CAP

    def ahead(i):
        return lax.rem(me + i * STEP, N_DEV)

    def behind(i):
        return lax.rem(me + i * (N_DEV - STEP), N_DEV)

    for c in tables:
        c.wait()

    def pick(i, _):
        p = ahead(i)
        for r in range(CAP):
            rows[i, r] = n_ref[jnp.clip(slot_s[0, p * CAP + r], 0, TOK - 1)]
        return 0

    def send_row(i, _):
        p = ahead(i)
        pltpu.make_async_remote_copy(rows.at[i], came.at[i], ss, rs.at[i // PER], device_id=dev(p), device_id_type=MESH).start()
        return 0

    lax.fori_loop(0, PER, pick, 0)
    came[0] = rows[0]
    pl.semaphore_wait(in_dp, 7)
    lax.fori_loop(1, PER, send_row, 0)
    for g in range(1, GROUPS):
        lax.fori_loop(g * PER, (g + 1) * PER, pick, 0)
        lax.fori_loop(g * PER, (g + 1) * PER, send_row, 0)
    for c in weights:
        c.wait()

    def group(g, _):
        base = g * PER

        def arrived(first, count, sem):
            part = pl.ds(first, count)
            pltpu.make_async_remote_copy(rows.at[part], came.at[part], ss, sem, device_id=dev(me), device_id_type=MESH).wait_recv()

        @pl.when(g == 0)
        def _():
            arrived(1, PER - 1, rs.at[0])

        @pl.when(g > 0)
        def _():
            arrived(base, PER, rs.at[g])

        def widen(t, _):
            for r in range(CAP):
                w3[t * CAP + r] = came[base + t, r].astype(F32)
            return 0

        lax.fori_loop(0, PER, widen, 0)
        for j in range(16):
            xs_v[:, j * HD:(j + 1) * HD] = w3[:, j, :].astype(BF)

        def up(k, _):
            xb = xs_v[...]
            a = jnp.minimum(jnp.dot(xb, wv[k, :, 0:256], preferred_element_type=F32), LIMIT)
            b = jnp.clip(jnp.dot(xb, wv[k, :, 256:512], preferred_element_type=F32), -LIMIT, LIMIT)
            act[k] = (a * jax.nn.sigmoid(SLOPE * a) * (b + 1.0)).astype(BF)
            return 0

        lax.fori_loop(0, 4, up, 0)

        for k in range(4):
            d = jnp.dot(act[0], wd[k, 0:256, :], preferred_element_type=F32)
            for m in range(1, 4):
                d = d + jnp.dot(act[m], wd[k, m * 256:(m + 1) * 256, :], preferred_element_type=F32)
            for j in range(4):
                w3[:, k * 4 + j, :] = d[:, j * HD:(j + 1) * HD]

        def narrow(t, _):
            for r in range(CAP):
                came[base + t, r] = w3[t * CAP + r].astype(BF)
            return 0

        lax.fori_loop(0, PER, narrow, 0)

        def answer(t, _):
            i = base + t
            pltpu.make_async_remote_copy(came.at[i], ret.at[me], ys, yr, device_id=dev(behind(i)), device_id_type=MESH).start()
            return 0

        @pl.when(g == 0)
        def _():
            ret[me] = came[0]
            lax.fori_loop(1, PER, answer, 0)

        @pl.when(g > 0)
        def _():
            lax.fori_loop(0, PER, answer, 0)

        return 0

    lax.fori_loop(0, GROUPS, group, 0)
    rest = pl.ds(0, N_DEV - 1)
    pltpu.make_async_remote_copy(came.at[rest], ret.at[rest], ys, yr, device_id=dev(me), device_id_type=MESH).wait()
    pltpu.make_async_remote_copy(rows.at[rest], came.at[rest], ss, rs.at[0], device_id=dev(me), device_id_type=MESH).wait_send()

    def token(t, _):
        for h in range(4):
            q = t * 4 + h
            i0, i1 = (jnp.clip(tgt_s[0, k], 0, N_DEV * CAP - 1) for k in (q, TOK + q))
            a = ret[i0 // CAP, lax.rem(i0, CAP)].astype(F32) * wt_ref[0, q]
            b = ret[i1 // CAP, lax.rem(i1, CAP)].astype(F32) * wt_ref[1, q]
            n3[q] = a + b
        return 0

    lax.fori_loop(0, TOK // 4, token, 0)
    for j in range(16):
        cols = slice(j * HD, (j + 1) * HD)
        o_ref[:, cols] = (u_ref[:, cols].astype(F32) + n3[:, j, :]).astype(BF)


def full(shape):
    return pl.BlockSpec(shape, lambda *i: (0,) * len(shape))


def per_device(resid, query, keys, values, q_gain, k_gain, out_weight, norm_gain, route_ids, route_weight,
               expert_gate, expert_up, expert_down):
    sds = jax.ShapeDtypeStruct
    sem = pltpu.SemaphoreType.DMA
    cosine, sine = turn_tables(lax.axis_index("sp"))
    ANY = pl.BlockSpec(memory_space=pl.ANY)
    V = pltpu.VMEM
    n = PER * CAP
    tiles = V((N_DEV, CAP, 16, HD), BF)
    out = pl.pallas_call(
        layer_kernel,
        out_shape=sds((TOK, 2048), BF),
        in_specs=[ANY] * 8 + [VM] * 6 + [SM], out_specs=VM,
        scratch_shapes=[V((TOK, 2048), BF), V((TOK, 512), BF), V((TOK, 512), BF), V((TOK, 2048), BF), V((4, 2048, 512), BF),
                        V((4, TOK, 512), BF), V((4, 2, TOK, HD), BF), V((4, TOK, 512), BF), V((4, 4, 2, TOK, HD), BF),
                        V((4, 1024, 256), BF), V((4, TOK, 512), BF), V((4, TOK, 512), BF), V((TOK, 16, HD), F32),
                        V((4, 1024, 256), F32), V((4, 1024, HD), F32), V((1, 2 * TOK), jnp.int32), V((1, N_DEV * CAP), jnp.int32),
                        pltpu.SMEM((1, 2 * TOK), jnp.int32), pltpu.SMEM((1, N_DEV * CAP), jnp.int32),
                        V((TOK, 2048), BF), V((TOK, 16, HD), BF), V((4, 1024, 512), BF),
                        tiles, tiles, tiles, V((n, 16, HD), F32), V((n, 2048), BF), V((4, n, 256), BF),
                        sem((8,)), sem((2,)), sem((3,)), sem((3,)), sem((3,)), sem((3,)), sem((2, 4)), sem((2, 4)), sem((4,)), sem((4,)),
                        sem((3,)), sem((3,)), sem((2, 2)), sem((2, 2)), sem((2,)), sem((2,)), sem((4,)), sem((4,)),
                        sem((12,)), sem, sem((GROUPS,)), sem, sem,
                        pltpu.SemaphoreType.REGULAR, pltpu.SemaphoreType.REGULAR],
        compiler_params=params(LIM * MB, cid=0), name="layer",
    )(query[0], keys[0], values[0], resid[0], out_weight, expert_gate[0], expert_up[0], expert_down[0],
      cosine, sine, q_gain[None], k_gain[None], norm_gain[None], route_ids[0].T, route_weight[0].T)
    return out[None]


def solution(mesh):
    placed = (
        P("dp", "sp", None),
        P("dp", "sp", None),
        P("dp", "sp", None),
        P("dp", "sp", None),
        P(),
        P(),
        P("dp", None),
        P(),
        P("dp", "sp", None),
        P("dp", "sp", None),
        P(("sp", "dp"), None, None),
        P(("sp", "dp"), None, None),
        P(("sp", "dp"), None, None),
    )
    return jax.shard_map(
        per_device, mesh=mesh, in_specs=placed, out_specs=P("dp", "sp", None), check_vma=False
    )
```

```python
import functools
import jax
import jax.numpy as jnp
from jax import lax
from jax.experimental import pallas as pl
from jax.experimental.pallas import tpu as pltpu
from jax.sharding import PartitionSpec as P

GRID_W = 64
EPSILON = 1e-06
THETA = 10000.0
LIMIT = 7.0
SLOPE = 1.702
LOG2E = 1.4426950408889634
HD = 128
TOK = 256
ZN = 4
XN = 4
N_DEV = 128
GROUPS = 4
PER = N_DEV // GROUPS
STEP = 37
CAP = 6
BF = jnp.bfloat16
F32 = jnp.float32
MESH = pl.DeviceIdType.MESH
VM = pl.BlockSpec(memory_space=pltpu.VMEM)
SM = pl.BlockSpec(memory_space=pltpu.SMEM)
MB = 1 << 20
LIM = 56


def params(limit=48 * MB, cid=None, **kw):
    if cid is not None:
        kw.update(collective_id=cid, has_side_effects=True)
    return pltpu.CompilerParams(vmem_limit_bytes=limit, **kw)


def turn_tables(sp):
    lane = jnp.arange(HD, dtype=jnp.int32)
    inverse = THETA ** (-(lane % 32).astype(F32) / 32)
    at = jnp.arange(GRID_W + 8, dtype=jnp.int32)
    place = jnp.where(at < GRID_W, at, sp * (TOK // GRID_W) + at - GRID_W)
    angles = place.astype(F32)[:, None] * inverse[None, :]
    sign = jnp.where(lane % 64 < 32, -1.0, 1.0)
    return jnp.cos(angles), jnp.sin(angles) * sign[None, :]


def per_token(table):
    lane = lax.broadcasted_iota(jnp.int32, (GRID_W, HD), 1)
    return jnp.concatenate(
        [jnp.where(lane < 64, table[GRID_W + b:GRID_W + b + 1, :], table[:GRID_W, :]) for b in range(TOK // GRID_W)], axis=0)


def turn_head(x, gain, cosine, sine, first):
    x = x.astype(F32)
    x = x * lax.rsqrt(jnp.mean(x * x, axis=-1, keepdims=True) + EPSILON) * gain
    other = jnp.where(first, pltpu.roll(x, HD - 32, 1), pltpu.roll(x, 32, 1))
    return (x * cosine + other * sine).astype(BF)


def sp_of(z, x):
    return {"sp": lax.rem(z, ZN) * XN + lax.rem(x, XN)}


def dp_of(y, c):
    return lax.rem(y, 4) * 2 + lax.rem(c, 2)


def route_tables(ids_ref, tgt_ref, slot_ref):
    n = 2 * TOK
    row = jnp.concatenate([ids_ref[0:1, :], ids_ref[1:2, :]], axis=1).astype(F32)
    ia = lax.broadcasted_iota(jnp.int32, (n, n), 0)
    ib = lax.broadcasted_iota(jnp.int32, (n, n), 1)
    col = jnp.sum(jnp.where(ia == ib, row, 0.0), axis=1, keepdims=True)
    same = col == row
    before = jnp.sum(jnp.where(same & (ia < ib), 1.0, 0.0), axis=0, keepdims=True)
    tgt_ref[...] = (row * CAP + before).astype(jnp.int32)
    before_c = jnp.sum(jnp.where(same & (ib < ia), 1.0, 0.0), axis=1, keepdims=True)
    target = (col * CAP + before_c).astype(jnp.int32)
    slots = lax.broadcasted_iota(jnp.int32, (n, N_DEV * CAP), 1)
    token = (lax.broadcasted_iota(jnp.int32, (n, N_DEV * CAP), 0) % TOK).astype(F32)
    slot_ref[...] = jnp.sum(jnp.where(target == slots, token, 0.0), axis=0, keepdims=True).astype(jnp.int32)


STEP_BLOCK = (3, 0, 0, 0, 1, 1, 1, 0, 1, 2, 2, 2, 2, 3, 3, 3)
STEP_QUARTER = (0, 0, 1, 3, 0, 1, 3, 2, 2, 0, 1, 3, 2, 1, 3, 2)


def step_entry(table, i):
    return sum(v * ((16 - lax.rem(i + 16 - k, 16)) // 16) for k, v in enumerate(table) if v)


def attend(q, kvr, ve, quarter, acc_ref, top_ref):
    scale = HD ** -0.5 * LOG2E
    q = jnp.concatenate([q[:, h * HD:(h + 1) * HD] for h in range(4)], axis=0)
    m, acc = jnp.max(top_ref[...], axis=-1, keepdims=True), acc_ref[...]
    for c in range(4):
        k = kvr[quarter, c, 0]
        s = lax.dot_general(q, k, (((1,), (1,)), ((), ())), preferred_element_type=F32)
        m_new = jnp.maximum(m, jnp.max(s, axis=-1, keepdims=True) * scale)
        p = jnp.exp2(s * scale - m_new).astype(BF)
        acc = acc * jnp.exp2(m - m_new) + jnp.dot(p, ve[quarter, c * TOK:(c + 1) * TOK, :], preferred_element_type=F32)
        m = m_new
    acc_ref[...] = acc
    top_ref[...] = jnp.broadcast_to(m, top_ref.shape)


def layer_kernel(q_hbm, k_hbm, v_hbm, r_hbm, w_hbm, wg_hbm, wu_hbm, wd_hbm, cos_ref, sin_ref, qg_ref, kg_ref, ng_ref, ids_ref, wt_ref,
                 o_ref,
                 qv, kx, vx, rv, wv, qs, kvs, qr, kvr, ve, heads, tok, n3, acc, tops, tgt_v, slot_v, tgt_s, slot_s,
                 u_ref, n_ref, wd, rows, came, ret, w3, xs_v, act,
                 ls, tsem, zks, zkr, zqs, zqr, xs, xr, fs, fr, hs, hr, w1s, w1r, w2s, w2r, wss, wsr, wsem, ss, rs, ys, yr, in_x, in_dp):
    sp, dp = lax.axis_index("sp"), lax.axis_index("dp")
    z, x = sp // XN, lax.rem(sp, XN)
    yy, core = dp // 2, lax.rem(dp, 2)
    me = sp * 8 + dp
    above, below, mate = dp_of(yy + 1, core), dp_of(yy + 3, core), dp_of(yy, core + 1)
    far_shard = dp_of(yy + 2, core)
    bar = pltpu.get_barrier_semaphore()

    def dev(p):
        return {"sp": p // 8, "dp": lax.rem(p, 8)}

    loads = {}
    for i, (name, src, dst) in enumerate((("k", k_hbm, kx), ("v", v_hbm, vx), ("q", q_hbm, qv), ("r", r_hbm, rv))):
        loads[name] = pltpu.make_async_copy(src, dst, ls.at[i])
        loads[name].start()

    w_loads = [pltpu.make_async_copy(w_hbm.at[:, nb * 512:(nb + 1) * 512], wv.at[nb, pl.ds(pl.multiple_of(dp * 256, 256), 256), :], ls.at[4 + nb])
               for nb in range(4)]
    for c in w_loads:
        c.start()

    def shard(p, half=None):
        if half is None:
            return wv.at[:, pl.ds(pl.multiple_of(p * 256, 256), 256), :]
        return wv.at[:, pl.ds(pl.multiple_of(p * 256 + half * 128, 128), 128), :]

    for d in (1, 2, 3):
        pl.semaphore_signal(bar, inc=1, device_id=sp_of(z + d, x), device_id_type=MESH)
        pl.semaphore_signal(bar, inc=1, device_id=sp_of(z, x + d), device_id_type=MESH)
    for d in range(1, 8):
        pl.semaphore_signal(bar, inc=1, device_id={"dp": lax.rem(dp + d, 8)}, device_id_type=MESH)
    weights = []
    for k in range(4):
        for src, dst in ((wg_hbm.at[:, k * 256:(k + 1) * 256], wv.at[k, :, 0:256]), (wu_hbm.at[:, k * 256:(k + 1) * 256], wv.at[k, :, 256:512]),
                         (wd_hbm.at[:, k * 512:(k + 1) * 512], wd.at[k])):
            weights.append(pltpu.make_async_copy(src, dst, wsem.at[len(weights)]))
    pending = []

    def remote(src, dst, ssem, rsem, dev):
        return pltpu.make_async_remote_copy(src, dst, ssem, rsem, device_id=dev, device_id_type=MESH)

    def send(src, dst, ssem, rsem, dev):
        c = remote(src, dst, ssem, rsem, dev)
        c.start()
        pending.append(c)
        return c

    pl.semaphore_wait(bar, 13)
    for d in (1, 2, 3):
        pl.semaphore_signal(in_x, inc=1, device_id=sp_of(z, x + d), device_id_type=MESH)
    for c in w_loads:
        c.wait()
    near_w = {}
    for half in (0, 1):
        for s, p in ((0, above), (1, below)):
            h = half if s == 0 else 1 - half
            near_w[s, h] = send(shard(dp, h), shard(dp, h), w1s.at[s, h], w1r.at[s, h], {"dp": p})
    mates = [send(shard(dp), shard(dp), wss.at[0], wsr.at[0], {"dp": mate})]
    first = lax.broadcasted_iota(jnp.int32, (TOK, HD), 1) % 64 < 32
    cosine, sine = per_token(cos_ref[...]), per_token(sin_ref[...])
    loads["k"].wait()
    loads["v"].wait()
    for h in range(4):
        kvs[h, 0] = turn_head(kx[:, h * HD:(h + 1) * HD], kg_ref[...], cosine, sine, first)
        kvs[h, 1] = vx[:, h * HD:(h + 1) * HD]
    zk = {}
    for d in (1, 3, 2):
        zk[d] = send(kvs.at[lax.rem(z + d, ZN)], kvr.at[x, z], zks.at[d - 1], zkr.at[d - 1], sp_of(z + d, x))
    kvr[x, z] = kvs[z]

    def gather(d):
        chunk = lax.rem(z + ZN - d, ZN)
        return [send(kvr.at[x, chunk], kvr.at[x, chunk], xs.at[s, d], xr.at[s, d], sp_of(z, x + (1, 3)[s])) for s in (0, 1)]

    near = {0: gather(0)}
    loads["q"].wait()

    def turn_query(d):
        zz = lax.rem(z + d, ZN)
        for h in range(4):
            cols = pl.ds(pl.multiple_of(zz * 512 + h * HD, HD), HD)
            val = turn_head(qv[:, cols], qg_ref[...], cosine, sine, first)
            if d:
                qs[zz, :, h * HD:(h + 1) * HD] = val
            else:
                qr[zz, :, h * HD:(h + 1) * HD] = val
        return zz

    for d in (3, 2, 1):
        zz = turn_query(d)
        send(qs.at[zz], qr.at[z], zqs.at[d - 1], zqr.at[d - 1], sp_of(z + d, x))
    def far_copy(d):
        chunk = lax.rem(z + ZN - d, ZN)
        s = 0 if d in (0, 1) else 1
        came_x = lax.rem(x + (3, 1)[s], XN)
        return remote(kvr.at[came_x, chunk], kvr.at[came_x, chunk], fs.at[d], fr.at[d], sp_of(z, x + (1, 3)[s]))

    def forward(d):
        near[d][0 if d in (0, 1) else 1].wait_recv()
        far_copy(d).start()

    far_w = [remote(shard(below, 0), shard(below, 0), w2s.at[0], w2r.at[0], {"dp": above}),
             remote(shard(above, 1), shard(above, 1), w2s.at[1], w2r.at[1], {"dp": below})]
    for c in weights[2::3]:
        c.start()
    route_tables(ids_ref, tgt_v, slot_v)
    tables = [pltpu.make_async_copy(tgt_v, tgt_s, tsem.at[0]), pltpu.make_async_copy(slot_v, slot_s, tsem.at[1])]
    for c in tables:
        c.start()
    pending += far_w + [far_copy(d) for d in range(4)]
    turn_query(0)
    pl.semaphore_wait(in_x, 3)
    for d in range(1, 8):
        pl.semaphore_signal(in_dp, inc=1, device_id={"dp": lax.rem(dp + d, 8)}, device_id_type=MESH)
    zk[1].wait_recv()
    near[1] = gather(1)
    zk[3].wait_recv()
    near[3] = gather(3)
    acc[...] = jnp.zeros_like(acc)
    tops[...] = jnp.full_like(tops, -jnp.inf)
    lane = lax.broadcasted_iota(jnp.int32, (1024, HD), 1)
    for c in range(4):
        ve[c, :, HD:] = jnp.where(lane == 0, 1.0, 0.0).astype(BF)
    zk[2].wait_recv()
    near[2] = gather(2)
    forward(0)

    def value_quarter(quarter):
        ve[quarter, :, :HD] = kvr[quarter, :, 1].reshape(1024, HD)

    value_quarter(x)

    def step(i, _):
        t, turn = step_entry(STEP_BLOCK, i), step_entry(STEP_QUARTER, i)
        a, quarter = lax.rem(z + 1 + t, ZN), lax.rem(x + ZN - turn, XN)

        @pl.when(i == 1)
        def _():
            forward(1)
            forward(3)

        @pl.when((i > 0) & (turn == 0))
        def _():
            remote(qs.at[a], qr.at[a], zqs.at[2 - t], zqr.at[2 - t], sp_of(a, x)).wait_recv()

        @pl.when(i == 2)
        def _():
            forward(2)
            near[2][0].wait_recv()
            near[3][0].wait_recv()
            value_quarter(quarter)

        @pl.when(i == 3)
        def _():
            near[0][1].wait_recv()
            near[1][1].wait_recv()
            value_quarter(quarter)

        @pl.when(i == 6)
        def _():
            near_w[0, 0].wait_recv()
            remote(shard(below, 0), shard(below, 0), w2s.at[0], w2r.at[0], {"dp": above}).start()
            near_w[1, 1].wait_recv()
            remote(shard(above, 1), shard(above, 1), w2s.at[1], w2r.at[1], {"dp": below}).start()

        @pl.when(i == 7)
        def _():
            for d in range(4):
                far_copy(d).wait_recv()
            value_quarter(quarter)

        attend(qr[a], kvr, ve, quarter, acc.at[t], tops.at[t])

        @pl.when(turn == 2)
        def _():
            done = acc[t]
            out = (done[:, :HD] / done[:, HD:HD + 1]).astype(BF)
            for h in range(4):
                heads[a, :, h * HD:(h + 1) * HD] = out[h * TOK:(h + 1) * TOK]

        @pl.when((turn == 2) & (t < 3))
        def _():
            remote(heads.at[a], tok.at[z], hs.at[t], hr.at[t], sp_of(a, x)).start()

        @pl.when(i == 11)
        def _():
            near_w[0, 1].wait_recv()
            remote(shard(below), shard(below), wss.at[1], wsr.at[1], {"dp": mate}).start()
            near_w[1, 0].wait_recv()
            remote(shard(above), shard(above), wss.at[2], wsr.at[2], {"dp": mate}).start()

        return 0

    lax.fori_loop(0, 16, step, 0)
    for c in far_w:
        c.wait_recv()
    remote(shard(far_shard), shard(far_shard), wss.at[3], wsr.at[3], {"dp": mate}).start()
    tok[z] = heads[z]
    for i in range(1, 4):
        c = remote(shard(dp), shard(dp), wss.at[i], wsr.at[i], {"dp": mate})
        pending.append(c)
        c.wait_recv()
    mates[0].wait_recv()
    loads["r"].wait()
    for t in range(3):
        c = remote(heads.at[t], tok.at[t], hs.at[t], hr.at[t], sp_of(z + 1, x))
        pending.append(c)
        c.wait_recv()
    for c in pending:
        c.wait_send()

    sq = None
    for nb in range(4):
        cols = slice(nb * 512, (nb + 1) * 512)
        acc = None
        for k in range(4):
            part = jnp.dot(tok[k], wv[nb, k * 512:(k + 1) * 512, :], preferred_element_type=F32)
            acc = part if acc is None else acc + part
        u = (rv[:, cols].astype(F32) + acc).astype(BF)
        u_ref[:, cols] = u
        wide = u.astype(F32)
        part = jnp.sum(wide * wide, axis=-1, keepdims=True)
        sq = part if sq is None else sq + part
    for i, c in enumerate(weights):
        if i % 3 < 2:
            c.start()
    inv = lax.rsqrt(sq / 2048.0 + EPSILON)
    for j in range(16):
        cols = slice(j * HD, (j + 1) * HD)
        n3[:, j, :] = u_ref[:, cols].astype(F32) * inv * ng_ref[:, cols]

    def narrow(t, _):
        rows = pl.ds(t * 8, 8)
        n_ref[rows] = n3[rows].astype(BF)
        return 0

    lax.fori_loop(0, TOK // 8, narrow, 0)

    n = PER * CAP

    def ahead(i):
        return lax.rem(me + i * STEP, N_DEV)

    def behind(i):
        return lax.rem(me + i * (N_DEV - STEP), N_DEV)

    for c in tables:
        c.wait()

    def pick(i, _):
        p = ahead(i)
        for r in range(CAP):
            rows[i, r] = n_ref[jnp.clip(slot_s[0, p * CAP + r], 0, TOK - 1)]
        return 0

    def send_row(i, _):
        p = ahead(i)
        pltpu.make_async_remote_copy(rows.at[i], came.at[i], ss, rs.at[i // PER], device_id=dev(p), device_id_type=MESH).start()
        return 0

    lax.fori_loop(0, PER, pick, 0)
    came[0] = rows[0]
    pl.semaphore_wait(in_dp, 7)
    lax.fori_loop(1, PER, send_row, 0)
    for g in range(1, GROUPS):
        lax.fori_loop(g * PER, (g + 1) * PER, pick, 0)
        lax.fori_loop(g * PER, (g + 1) * PER, send_row, 0)
    for c in weights:
        c.wait()

    def group(g, _):
        base = g * PER

        def arrived(first, count, sem):
            part = pl.ds(first, count)
            pltpu.make_async_remote_copy(rows.at[part], came.at[part], ss, sem, device_id=dev(me), device_id_type=MESH).wait_recv()

        @pl.when(g == 0)
        def _():
            arrived(1, PER - 1, rs.at[0])

        @pl.when(g > 0)
        def _():
            arrived(base, PER, rs.at[g])

        def widen(t, _):
            for r in range(CAP):
                w3[t * CAP + r] = came[base + t, r].astype(F32)
            return 0

        lax.fori_loop(0, PER, widen, 0)
        for j in range(16):
            xs_v[:, j * HD:(j + 1) * HD] = w3[:, j, :].astype(BF)

        def up(k, _):
            xb = xs_v[...]
            a = jnp.minimum(jnp.dot(xb, wv[k, :, 0:256], preferred_element_type=F32), LIMIT)
            b = jnp.clip(jnp.dot(xb, wv[k, :, 256:512], preferred_element_type=F32), -LIMIT, LIMIT)
            act[k] = (a * jax.nn.sigmoid(SLOPE * a) * (b + 1.0)).astype(BF)
            return 0

        lax.fori_loop(0, 4, up, 0)

        for k in range(4):
            d = jnp.dot(act[0], wd[k, 0:256, :], preferred_element_type=F32)
            for m in range(1, 4):
                d = d + jnp.dot(act[m], wd[k, m * 256:(m + 1) * 256, :], preferred_element_type=F32)
            for j in range(4):
                w3[:, k * 4 + j, :] = d[:, j * HD:(j + 1) * HD]

        def narrow(t, _):
            for r in range(CAP):
                came[base + t, r] = w3[t * CAP + r].astype(BF)
            return 0

        lax.fori_loop(0, PER, narrow, 0)

        def answer(t, _):
            i = base + t
            pltpu.make_async_remote_copy(came.at[i], ret.at[me], ys, yr, device_id=dev(behind(i)), device_id_type=MESH).start()
            return 0

        @pl.when(g == 0)
        def _():
            ret[me] = came[0]
            lax.fori_loop(1, PER, answer, 0)

        @pl.when(g > 0)
        def _():
            lax.fori_loop(0, PER, answer, 0)

        return 0

    lax.fori_loop(0, GROUPS, group, 0)
    rest = pl.ds(0, N_DEV - 1)
    pltpu.make_async_remote_copy(came.at[rest], ret.at[rest], ys, yr, device_id=dev(me), device_id_type=MESH).wait()
    pltpu.make_async_remote_copy(rows.at[rest], came.at[rest], ss, rs.at[0], device_id=dev(me), device_id_type=MESH).wait_send()

    def token(t, _):
        for h in range(4):
            q = t * 4 + h
            i0, i1 = (jnp.clip(tgt_s[0, k], 0, N_DEV * CAP - 1) for k in (q, TOK + q))
            a = ret[i0 // CAP, lax.rem(i0, CAP)].astype(F32) * wt_ref[0, q]
            b = ret[i1 // CAP, lax.rem(i1, CAP)].astype(F32) * wt_ref[1, q]
            n3[q] = a + b
        return 0

    lax.fori_loop(0, TOK // 4, token, 0)
    for j in range(16):
        cols = slice(j * HD, (j + 1) * HD)
        o_ref[:, cols] = (u_ref[:, cols].astype(F32) + n3[:, j, :]).astype(BF)


def full(shape):
    return pl.BlockSpec(shape, lambda *i: (0,) * len(shape))


def per_device(resid, query, keys, values, q_gain, k_gain, out_weight, norm_gain, route_ids, route_weight,
               expert_gate, expert_up, expert_down):
    sds = jax.ShapeDtypeStruct
    sem = pltpu.SemaphoreType.DMA
    cosine, sine = turn_tables(lax.axis_index("sp"))
    ANY = pl.BlockSpec(memory_space=pl.ANY)
    V = pltpu.VMEM
    n = PER * CAP
    tiles = V((N_DEV, CAP, 16, HD), BF)
    out = pl.pallas_call(
        layer_kernel,
        out_shape=sds((TOK, 2048), BF),
        in_specs=[ANY] * 8 + [VM] * 6 + [SM], out_specs=VM,
        scratch_shapes=[V((TOK, 2048), BF), V((TOK, 512), BF), V((TOK, 512), BF), V((TOK, 2048), BF), V((4, 2048, 512), BF),
                        V((4, TOK, 512), BF), V((4, 2, TOK, HD), BF), V((4, TOK, 512), BF), V((4, 4, 2, TOK, HD), BF),
                        V((4, 1024, 256), BF), V((4, TOK, 512), BF), V((4, TOK, 512), BF), V((TOK, 16, HD), F32),
                        V((4, 1024, 256), F32), V((4, 1024, HD), F32), V((1, 2 * TOK), jnp.int32), V((1, N_DEV * CAP), jnp.int32),
                        pltpu.SMEM((1, 2 * TOK), jnp.int32), pltpu.SMEM((1, N_DEV * CAP), jnp.int32),
                        V((TOK, 2048), BF), V((TOK, 16, HD), BF), V((4, 1024, 512), BF),
                        tiles, tiles, tiles, V((n, 16, HD), F32), V((n, 2048), BF), V((4, n, 256), BF),
                        sem((8,)), sem((2,)), sem((3,)), sem((3,)), sem((3,)), sem((3,)), sem((2, 4)), sem((2, 4)), sem((4,)), sem((4,)),
                        sem((3,)), sem((3,)), sem((2, 2)), sem((2, 2)), sem((2,)), sem((2,)), sem((4,)), sem((4,)),
                        sem((12,)), sem, sem((GROUPS,)), sem, sem,
                        pltpu.SemaphoreType.REGULAR, pltpu.SemaphoreType.REGULAR],
        compiler_params=params(LIM * MB, cid=0), name="layer",
    )(query[0], keys[0], values[0], resid[0], out_weight, expert_gate[0], expert_up[0], expert_down[0],
      cosine, sine, q_gain[None], k_gain[None], norm_gain[None], route_ids[0].T, route_weight[0].T)
    return out[None]


def solution(mesh):
    placed = (
        P("dp", "sp", None),
        P("dp", "sp", None),
        P("dp", "sp", None),
        P("dp", "sp", None),
        P(),
        P(),
        P("dp", None),
        P(),
        P("dp", "sp", None),
        P("dp", "sp", None),
        P(("sp", "dp"), None, None),
        P(("sp", "dp"), None, None),
        P(("sp", "dp"), None, None),
    )
    return jax.shard_map(
        per_device, mesh=mesh, in_specs=placed, out_specs=P("dp", "sp", None), check_vma=False
    )
```
